32 devices in a mesh: rep: 2 (over y), fs: 4 (over z), tp: 4 (over x, core).
Axes of the slice: x: 2, y: 2, z: 4, core: 2. Of those that a mesh axis runs over, the one named last changes fastest.
Arguments:
- tokens: bfloat16 [4096, 2048], P(('rep', 'fs')), may hold values from -6 to 6
- norm_gain: float32 [2048], replicated, may hold values from 0.1 to 1.9
- up_weight: bfloat16 [2048, 4096], P('fs', 'tp'), may hold values from -0.125 to 0.125
- down_weight: bfloat16 [4096, 2048], P('tp', 'fs'), may hold values from -0.09375 to 0.09375
Outputs:
- result: bfloat16 [4096, 2048], P(('rep', 'fs', 'tp'))
The draws below stay inside these ranges and needn't reach their ends.
All inputs are finite; a program needn't handle non-finite values.
Results may differ from the reference program's by a relative error of at most 0.012.
Values may be sent and summed in bfloat16 or wider, within the bound.
A program may use at most 64 MiB of HBM per device.

```python
import jax
import jax.numpy as jnp
from jax import lax

D = 2048
FF = 4096
TOKENS = 4096
N_TP = 4


def block_scale(own_key, dims, split, smallest, largest):
    loudness = 1.0
    for axis_at, parts in split:
        draws = jax.random.uniform(jax.random.fold_in(jax.random.fold_in(own_key, 6), axis_at), (parts,), jnp.float32, smallest / len(split), largest / len(split))
        loudness = loudness * jnp.repeat(jnp.exp(draws), dims[axis_at] // parts).reshape((-1,) + (1,) * (len(dims) - 1 - axis_at))
    return loudness


def normal_values(key, shape, spread, most, pieces=(), held_as=jnp.bfloat16):
    level = block_scale(key, shape, pieces, -0.22, 0.18) if pieces else 1.0
    drawn = jax.random.normal(key, shape, jnp.float32) * spread * level
    return jnp.minimum(jnp.maximum(drawn, -most), most).astype(held_as)


def setup_inputs(seed: int = 0) -> dict:
    key_list = jax.random.split(jax.random.key(seed), 5)
    return {
        "tokens": normal_values(key_list[0], (TOKENS, D), 1.0, 6.0, ((0, 8),)),
        "norm_gain": jnp.clip(1.0 + 0.18 * jax.random.normal(key_list[1], (D,), jnp.float32), 0.1, 1.9),
        "up_weight": normal_values(key_list[2], (D, FF), D ** -0.5, 0.125, ((0, 4), (1, 4))),
        "down_weight": normal_values(key_list[3], (FF, D), FF ** -0.5, 0.09375, ((0, 4), (1, 4))),
    }


EPS = 1e-06

def reference(tokens, norm_gain, up_weight, down_weight):
    xf = tokens.astype(jnp.float32)
    scale = lax.rsqrt(lax.optimization_barrier(jnp.mean(xf * xf, axis=-1, keepdims=True)) + EPS)
    normed = (xf * scale * norm_gain.astype(jnp.float32)).astype(jnp.bfloat16)
    lifted = jnp.dot(normed, up_weight, preferred_element_type=jnp.float32)
    hidden = jnp.square(jnp.maximum(lifted, 0.0)).astype(jnp.bfloat16)
    block = FF // N_TP
    total = xf
    for index in range(N_TP):
        part = jnp.dot(hidden[:, index * block:(index + 1) * block], down_weight[index * block:(index + 1) * block, :], preferred_element_type=jnp.float32)
        rounded = lax.optimization_barrier(part.astype(jnp.bfloat16))
        total = total + rounded.astype(jnp.float32)
    return total.astype(jnp.bfloat16)
```

```python
import functools

import jax
import jax.numpy as jnp
from jax import lax
from jax.experimental import pallas as pl
from jax.experimental.pallas import tpu as pltpu
from jax.sharding import PartitionSpec as P

EPS = 1e-06
UP_PIECES = 8
DN_CHUNKS = 2
DN_PIECES = 4
TOK_PIECES = 2
BESIDE = 2
LAG = 2


def shards(tokens, norm_gain, up_weight, down_weight):
    xf = tokens.astype(jnp.float32)
    scale = lax.rsqrt(jnp.mean(xf * xf, axis=-1, keepdims=True) + EPS)
    normed = (xf * scale * norm_gain).astype(jnp.bfloat16)
    rows = tokens.shape[0]
    halves = lax.axis_size("rep")
    share = up_weight.shape[0] // halves
    mine = lax.dynamic_slice_in_dim(up_weight, lax.axis_index("rep") * share, share, 0)
    arranged = normed.reshape(rows, -1, halves, share).transpose(0, 2, 1, 3).reshape(rows, -1)
    lifted = jnp.dot(
        arranged,
        lax.all_gather(mine, ("rep", "fs"), axis=0, tiled=True),
        preferred_element_type=jnp.float32,
    )
    width = down_weight.shape[1] // halves
    down_mine = lax.dynamic_slice_in_dim(down_weight, lax.axis_index("rep") * width, width, 1)
    collected = lax.all_gather(down_mine, ("rep", "fs"), axis=1, tiled=True)
    hidden_rows = collected.shape[0]
    down_block = (
        collected.reshape(hidden_rows, halves, -1, width)
        .transpose(0, 2, 1, 3)
        .reshape(hidden_rows, -1)
    )
    hidden = jnp.square(jnp.maximum(lifted, 0.0)).astype(jnp.bfloat16)
    own_rows = rows // lax.axis_size("tp")
    summed = lax.psum_scatter(
        jnp.dot(hidden, down_block, preferred_element_type=jnp.float32).astype(jnp.bfloat16),
        "tp",
        scatter_dimension=0,
        tiled=True,
    ).astype(jnp.float32)
    residual = lax.dynamic_slice_in_dim(xf, lax.axis_index("tp") * own_rows, own_rows, 0)
    return (residual + summed).astype(jnp.bfloat16)


def kernel(
    n, tok_hbm, gain_hbm, up_hbm, dn_hbm, out_hbm,
    gain_ref, tok, nrm, upw, dnw, lifted, hid, part, asend, arecv, bsend, brecv, keep, outv,
    up_send, up_recv, dn_send, dn_recv, t_send, t_recv,
    a_send, a_recv, b_send, b_recv, o_send, o_recv, local,
):
    y, z, t = lax.axis_index("rep"), lax.axis_index("fs"), lax.axis_index("tp")
    x, core = t // 2, t % 2
    rows = tok_hbm.shape[0]
    own_rows = rows // 4
    up_rows, H = up_hbm.shape
    CW = dnw.shape[2]
    UP, DC, DP, TP = UP_PIECES, DN_CHUNKS, DN_PIECES, TOK_PIECES
    UM, DM = UP // 2, DP // 2
    piece, depth, band = up_rows // UP, H // DP, own_rows // TP
    chunks = n * DC

    is_outer = (z == 0) | (z == n - 1)
    outer = jnp.where(z < n // 2, 0, n - 1)
    inner = jnp.where(z < n // 2, n // 2 - 1, n // 2)
    mate = n - 1 - z
    far = n - 1 - outer

    def at(yy, zz, tt):
        return {"rep": yy, "fs": zz, "tp": tt}

    PARTNER = at(y, z, x * 2 + (1 - core))
    ASIDE = at(y, z, (1 - x) * 2 + core)
    ACROSS = at(1 - y, z, t)
    MATE = at(y, mate, t)
    OUTER = at(y, outer, t)
    INNER = at(y, inner, t)

    def remote(src, dst, send, recv, where):
        return pltpu.make_async_remote_copy(
            src_ref=src, dst_ref=dst, send_sem=send, recv_sem=recv,
            device_id=where, device_id_type=pl.DeviceIdType.MESH,
        )

    def up_slot(s, p):
        return upw.at[pl.ds(pl.multiple_of(s * up_rows + p * piece, piece), piece), :]

    def up_own(p):
        return up_hbm.at[pl.ds(pl.multiple_of(p * piece, piece), piece), :]

    def dn_slot(s, j, k):
        return dnw.at[s * DC + j, pl.ds(pl.multiple_of(k * depth, depth), depth), :]

    def dn_own(j, k):
        return dn_hbm.at[pl.ds(pl.multiple_of(k * depth, depth), depth), pl.ds(j * CW, CW)]

    def up_copy(side, s, p, src, where):
        return remote(src, up_slot(s, p), up_send.at[side, s * UP + p], up_recv.at[s * UP + p], where)

    def dn_copy(side, s, j, k, src, where):
        q = (s * DC + j) * DP + k
        return remote(src, dn_slot(s, j, k), dn_send.at[side, q], dn_recv.at[q], where)

    def up_landed(s, p):
        up_copy(0, s, p, up_slot(s, p), MATE).wait_recv()

    def dn_landed(s, j, k):
        dn_copy(0, s, j, k, dn_slot(s, j, k), MATE).wait_recv()

    def tok_slot(q, b):
        return tok.at[1, pl.ds(pl.multiple_of(q * own_rows + b * band, band), band), :]

    def tok_copy(side, q, b, src, where):
        return remote(src, tok_slot(q, b), t_send.at[side, b], t_recv.at[side, b], where)

    def out_cols(s, j):
        return out_hbm.at[:, pl.ds(pl.multiple_of((s * DC + j) * CW, CW), CW)]

    barrier = pltpu.get_barrier_semaphore()

    def greet(peers):
        for peer in peers:
            pl.semaphore_signal(barrier, inc=1, device_id=peer, device_id_type=pl.DeviceIdType.MESH)

    mine_up, other_up = y * UM, (1 - y) * UM
    mine_dn, other_dn = y * DM, (1 - y) * DM

    @pl.when(is_outer)
    def _():
        greet([INNER])
        pl.semaphore_wait(barrier, 1)
        copies = []
        for p in range(UM):
            copies.append(up_copy(0, z, mine_up + p, up_own(mine_up + p), INNER))
        for b in range(TP):
            own = tok_hbm.at[pl.ds(pl.multiple_of(t * own_rows + b * band, band), band), :]
            copies.append(tok_copy(0, t, b, own, INNER))
        for p in range(UM - BESIDE):
            copies.append(up_copy(0, z, other_up + p, up_own(other_up + p), INNER))
        for first in (mine_dn, other_dn):
            for j in range(DC):
                for k in range(DM):
                    copies.append(dn_copy(0, z, j, first + k, dn_own(j, first + k), INNER))
        for copy in copies:
            copy.start()
        for copy in copies:
            copy.wait_send()
        for s in range(n):
            for j in range(DC):
                q = s * DC + j
                remote(outv.at[1, q], out_cols(s, j), o_send.at[q], o_recv.at[q], INNER).wait_recv()

    @pl.when(jnp.logical_not(is_outer))
    def _():
        greet([PARTNER, ASIDE, ACROSS, MATE, OUTER])
        tok_load = pltpu.make_async_copy(tok_hbm, tok.at[0], local.at[0])
        gain_load = pltpu.make_async_copy(gain_hbm, gain_ref, local.at[1])
        up_load = pltpu.make_async_copy(
            up_hbm, upw.at[pl.ds(pl.multiple_of(z * up_rows, up_rows), up_rows), :], local.at[2]
        )
        dn_loads = [
            pltpu.make_async_copy(dn_hbm.at[:, pl.ds(j * CW, CW)], dnw.at[z * DC + j], local.at[3 + j])
            for j in range(DC)
        ]
        for load in [gain_load, tok_load, up_load] + dn_loads:
            load.start()
        pl.semaphore_wait(barrier, 5)

        for p in range(UM):
            up_copy(0, z, mine_up + p, up_own(mine_up + p), MATE).start()

        gain_load.wait()
        gain = gain_ref[...]

        def normalise(src, q):
            xf = tok[src, pl.ds(pl.multiple_of(q * own_rows, own_rows), own_rows), :].astype(jnp.float32)
            scale = lax.rsqrt(jnp.mean(xf * xf, axis=-1, keepdims=True) + EPS)
            to = (q % 2 * 2 + q // 2) * own_rows
            nrm[src, pl.ds(pl.multiple_of(to, own_rows), own_rows), :] = (xf * scale * gain).astype(jnp.bfloat16)

        def lift(src, s, first=False, last=False):
            def half(i, carry):
                r = pl.ds(pl.multiple_of(i * (rows // 2), rows // 2), rows // 2)
                k = pl.ds(pl.multiple_of(s * up_rows, up_rows), up_rows)
                value = jnp.dot(nrm[src, r, k], upw[k, :], preferred_element_type=jnp.float32)
                if not first:
                    value = value + lifted[src, r, :]
                if last:
                    hid[src, i] = jnp.square(jnp.maximum(value, 0.0)).astype(jnp.bfloat16)
                else:
                    lifted[src, r, :] = value
                return carry
            lax.fori_loop(0, 2, half, 0)

        tok_load.wait()
        lax.fori_loop(0, 4, lambda q, carry: (normalise(0, q), carry)[1], 0)
        up_load.wait()

        def relay_near(p, carry):
            up_landed(outer, mine_up + p)
            up_copy(0, outer, mine_up + p, up_slot(outer, mine_up + p), MATE).start()

            @pl.when(p >= UM - BESIDE)
            def _():
                up_copy(1, outer, mine_up + p, up_slot(outer, mine_up + p), ACROSS).start()

            up_landed(mate, mine_up + p)
            up_copy(1, mate, mine_up + p, up_slot(mate, mine_up + p), ACROSS).start()
            return carry

        lax.fori_loop(0, 1, relay_near, 0)
        lift(0, z, first=True)
        lax.fori_loop(1, UM, relay_near, 0)
        for j in range(DC):
            dn_loads[j].wait()
            for k in range(DM):
                dn_copy(0, z, j, mine_dn + k, dn_own(j, mine_dn + k), MATE).start()

        def relay_far(p):
            up_landed(far, mine_up + p)
            up_copy(1, far, mine_up + p, up_slot(far, mine_up + p), ACROSS).start()

        beyond = (1 - x) * 2 + core
        for b in range(TP):
            for p in range(b * UM // TP, (b + 1) * UM // TP):
                relay_far(p)
            tok_copy(0, t, b, tok_slot(t, b), INNER).wait_recv()
            tok_copy(1, t, b, tok_slot(t, b), ASIDE).start()
            tok_copy(2, t, b, tok_slot(t, b), PARTNER).start()
        for p in range(UM):
            up_landed(mate, other_up + p)
        lift(0, mate)
        normalise(1, t)
        for b in range(TP):
            tok_copy(1, beyond, b, tok_slot(beyond, b), ASIDE).wait_recv()
            tok_copy(3, beyond, b, tok_slot(beyond, b), PARTNER).start()
        for b in range(TP):
            tok_copy(2, x * 2 + 1 - core, b, tok_slot(x * 2 + 1 - core, b), PARTNER).wait_recv()
        normalise(1, x * 2 + 1 - core)
        normalise(1, beyond)
        for b in range(TP):
            tok_copy(3, (1 - x) * 2 + 1 - core, b, tok_slot((1 - x) * 2 + 1 - core, b), PARTNER).wait_recv()
        normalise(1, (1 - x) * 2 + 1 - core)
        lift(1, z, first=True)
        lift(1, mate)
        for p in range(UM):
            up_landed(outer, other_up + p)
        lift(0, outer)

        def relay_dn(s, j, side, where):
            for k in range(DM):
                dn_landed(s, j, mine_dn + k)
                dn_copy(side, s, j, mine_dn + k, dn_slot(s, j, mine_dn + k), where).start()

        relay_dn(mate, 0, 1, ACROSS)
        lift(1, outer)
        for p in range(UM):
            up_landed(far, other_up + p)
        lift(0, far, last=True)
        lift(1, far, last=True)

        order = [(z, 0), (z, 1), (mate, 0), (mate, 1), (outer, 0), (far, 0), (outer, 1), (far, 1)]

        def a_copy(i):
            return remote(asend.at[i], arecv.at[i], a_send.at[i], a_recv.at[i], PARTNER)

        def b_copy(i):
            return remote(bsend.at[i], brecv.at[i], b_send.at[i], b_recv.at[i], ASIDE)

        def own_copy(i):
            s, j = order[i]
            return pltpu.make_async_copy(outv.at[0, s * DC + j], out_cols(s, j), local.at[3 + DC + i])

        def out_copy(i):
            s, j = order[i]
            q = s * DC + j
            return remote(outv.at[1, q], out_cols(s, j), o_send.at[q], o_recv.at[q], OUTER)

        def compute(i):
            s, j = order[i]
            block = dnw[s * DC + j]
            theirs = hid[:, 1 - core].reshape(rows, H)
            sent = jnp.dot(theirs, block, preferred_element_type=jnp.float32).astype(jnp.bfloat16)
            asend[i] = sent.reshape(2, 2, own_rows, CW)
            a_copy(i).start()
            ours = hid[:, core].reshape(rows, H)
            part[i % 2] = jnp.dot(ours, block, preferred_element_type=jnp.float32).reshape(2, 2, own_rows, CW)

        def join(i):
            a_copy(i).wait_recv()
            bsend[i] = (part[i % 2, :, 1 - x] + arecv[i, :, 1 - x].astype(jnp.float32)).astype(jnp.bfloat16)
            b_copy(i).start()
            keep[i] = part[i % 2, :, x] + arecv[i, :, x].astype(jnp.float32)

        def finish(i):
            s, j = order[i]
            q = s * DC + j
            b_copy(i).wait_recv()
            r = pl.ds(pl.multiple_of(t * own_rows, own_rows), own_rows)
            c = pl.ds(pl.multiple_of(q * CW, CW), CW)
            for src in (1, 0):
                res = tok[src, r, c].astype(jnp.float32) + keep[i, src] + brecv[i, src].astype(jnp.float32)
                outv[src, q] = res.astype(jnp.bfloat16)
                (own_copy if src == 0 else out_copy)(i).start()

        def arrive(s, j):
            for k in range(DM):
                dn_landed(s, j, other_dn + k)

        def own_arrive(s, j):
            for k in range(DM):
                dn_landed(s, j, mine_dn + k)

        before = {
            1: [lambda: relay_dn(mate, 1, 1, ACROSS), lambda: relay_dn(outer, 0, 0, MATE)],
            2: [lambda: arrive(mate, 0)],
            3: [lambda: relay_dn(outer, 1, 0, MATE), lambda: relay_dn(far, 0, 1, ACROSS), lambda: arrive(mate, 1)],
            4: [lambda: arrive(outer, 0)],
            5: [lambda: relay_dn(far, 1, 1, ACROSS), lambda: arrive(far, 0)],
            6: [lambda: arrive(outer, 1)],
            7: [lambda: arrive(far, 1)],
        }
        for i in range(chunks):
            for act in before.get(i, []):
                act()
            compute(i)
            if i > 0:
                join(i - 1)
            if i >= LAG:
                finish(i - LAG)
        join(chunks - 1)
        for i in range(chunks - LAG, chunks):
            finish(i)

        for p in range(UM):
            for side, s in ((0, z), (0, outer), (1, mate), (1, far)):
                up_copy(side, s, mine_up + p, up_slot(s, mine_up + p), MATE).wait_send()
            if p >= UM - BESIDE:
                up_copy(1, outer, mine_up + p, up_slot(outer, mine_up + p), MATE).wait_send()
        for b in range(TP):
            for side in (1, 2, 3):
                tok_copy(side, t, b, tok_slot(t, b), PARTNER).wait_send()
        for side, s in ((0, z), (0, outer), (1, mate), (1, far)):
            for j in range(DC):
                for k in range(DM):
                    dn_copy(side, s, j, mine_dn + k, dn_slot(s, j, mine_dn + k), MATE).wait_send()
        for i in range(chunks):
            a_copy(i).wait_send()
            b_copy(i).wait_send()
            own_copy(i).wait()
            out_copy(i).wait_send()


def fused(n, tokens, norm_gain, up_weight, down_weight):
    rows, D = tokens.shape
    up_rows, H = up_weight.shape
    CW = down_weight.shape[1] // DN_CHUNKS
    chunks = n * DN_CHUNKS
    own_rows = rows // 4
    bf, f32 = jnp.bfloat16, jnp.float32
    dma = pltpu.SemaphoreType.DMA
    return pl.pallas_call(
        functools.partial(kernel, n),
        out_shape=jax.ShapeDtypeStruct((own_rows, D), bf),
        in_specs=[pl.BlockSpec(memory_space=pl.ANY)] * 4,
        out_specs=pl.BlockSpec(memory_space=pl.ANY),
        scratch_shapes=[
            pltpu.VMEM((1, D), f32),
            pltpu.VMEM((2, rows, D), bf),
            pltpu.VMEM((2, rows, D), bf),
            pltpu.VMEM((n * up_rows, H), bf),
            pltpu.VMEM((chunks, H, CW), bf),
            pltpu.VMEM((2, rows, H), f32),
            pltpu.VMEM((2, 2, rows // 2, H), bf),
            pltpu.VMEM((2, 2, 2, own_rows, CW), f32),
            pltpu.VMEM((chunks, 2, 2, own_rows, CW), bf),
            pltpu.VMEM((chunks, 2, 2, own_rows, CW), bf),
            pltpu.VMEM((chunks, 2, own_rows, CW), bf),
            pltpu.VMEM((chunks, 2, own_rows, CW), bf),
            pltpu.VMEM((chunks, 2, own_rows, CW), f32),
            pltpu.VMEM((2, chunks, own_rows, CW), bf),
            dma((2, n * UP_PIECES)),
            dma((n * UP_PIECES,)),
            dma((2, chunks * DN_PIECES)),
            dma((chunks * DN_PIECES,)),
            dma((4, TOK_PIECES)),
            dma((4, TOK_PIECES)),
            dma((chunks,)),
            dma((chunks,)),
            dma((chunks,)),
            dma((chunks,)),
            dma((chunks,)),
            dma((chunks,)),
            dma((3 + DN_CHUNKS + chunks,)),
        ],
        compiler_params=pltpu.CompilerParams(
            collective_id=0, has_side_effects=True, vmem_limit_bytes=53 * 1024 * 1024
        ),
    )(tokens, norm_gain.reshape(1, D), up_weight, down_weight)


def fits(mesh, tokens, up_weight, down_weight):
    n = mesh.shape["fs"]
    rows = tokens.shape[0] // (mesh.shape["rep"] * n)
    columns = down_weight.shape[1] // n
    depth = up_weight.shape[0] // n
    hidden = up_weight.shape[1] // mesh.shape["tp"]
    return (
        mesh.shape["rep"] == 2
        and mesh.shape["tp"] == 4
        and n == 4
        and columns % (128 * DN_CHUNKS) == 0
        and depth % (UP_PIECES * 16) == 0
        and depth % 128 == 0
        and hidden % (16 * DN_PIECES) == 0
        and hidden % 128 == 0
        and rows % (4 * 16 * TOK_PIECES) == 0
        and rows <= 512
        and hidden <= 1024
        and tokens.shape[1] <= 2048
    )


def solution(mesh):
    placed = (P(("rep", "fs"), None), P(), P("fs", "tp"), P("tp", "fs"))

    def layer(tokens, norm_gain, up_weight, down_weight):
        if fits(mesh, tokens, up_weight, down_weight):
            body = functools.partial(fused, mesh.shape["fs"])
        else:
            body = shards
        return jax.shard_map(
            body, mesh=mesh, in_specs=placed, out_specs=P(("rep", "fs", "tp"), None), check_vma=False
        )(tokens, norm_gain, up_weight, down_weight)

    return layer
```

```python
import functools

import jax
import jax.numpy as jnp
from jax import lax
from jax.experimental import pallas as pl
from jax.experimental.pallas import tpu as pltpu
from jax.sharding import PartitionSpec as P

EPS = 1e-06
UP_PIECES = 16
DN_CHUNKS = 2
DN_PIECES = 8
TOK_PIECES = 4
BESIDE = 4
VIA_MATE = 2
LAG = 4
ORDER = (
    ("inner", 0), ("inner", 1), ("mate", 0), ("mate", 1),
    ("outer", 0), ("far", 0), ("outer", 1), ("far", 1),
)
DIRECT = (1, 3, 5, 7)


def shards(tokens, norm_gain, up_weight, down_weight):
    xf = tokens.astype(jnp.float32)
    scale = lax.rsqrt(jnp.mean(xf * xf, axis=-1, keepdims=True) + EPS)
    normed = (xf * scale * norm_gain).astype(jnp.bfloat16)
    rows = tokens.shape[0]
    halves = lax.axis_size("rep")
    share = up_weight.shape[0] // halves
    mine = lax.dynamic_slice_in_dim(up_weight, lax.axis_index("rep") * share, share, 0)
    arranged = normed.reshape(rows, -1, halves, share).transpose(0, 2, 1, 3).reshape(rows, -1)
    lifted = jnp.dot(
        arranged,
        lax.all_gather(mine, ("rep", "fs"), axis=0, tiled=True),
        preferred_element_type=jnp.float32,
    )
    width = down_weight.shape[1] // halves
    down_mine = lax.dynamic_slice_in_dim(down_weight, lax.axis_index("rep") * width, width, 1)
    collected = lax.all_gather(down_mine, ("rep", "fs"), axis=1, tiled=True)
    hidden_rows = collected.shape[0]
    down_block = (
        collected.reshape(hidden_rows, halves, -1, width)
        .transpose(0, 2, 1, 3)
        .reshape(hidden_rows, -1)
    )
    hidden = jnp.square(jnp.maximum(lifted, 0.0)).astype(jnp.bfloat16)
    own_rows = rows // lax.axis_size("tp")
    summed = lax.psum_scatter(
        jnp.dot(hidden, down_block, preferred_element_type=jnp.float32).astype(jnp.bfloat16),
        "tp",
        scatter_dimension=0,
        tiled=True,
    ).astype(jnp.float32)
    residual = lax.dynamic_slice_in_dim(xf, lax.axis_index("tp") * own_rows, own_rows, 0)
    return (residual + summed).astype(jnp.bfloat16)


def kernel(
    n, tok_hbm, gain_hbm, up_hbm, dn_hbm, out_hbm,
    gain_ref, tok, nrm, upw, dnw, lifted, hid, part, asend, arecv, bsend, brecv, keep, outv, dsend, drecv,
    up_send, up_recv, dn_send, dn_recv, t_send, t_recv,
    a_send, a_recv, b_send, b_recv, o_send, o_recv, d_send, d_recv, own_sem, local,
):
    y, z, t = lax.axis_index("rep"), lax.axis_index("fs"), lax.axis_index("tp")
    x, core = t // 2, t % 2
    rows = tok_hbm.shape[0]
    own_rows = rows // 4
    up_rows, H = up_hbm.shape
    CW = dnw.shape[2]
    UP, DC, DP, TP = UP_PIECES, DN_CHUNKS, DN_PIECES, TOK_PIECES
    UM, DM = UP // 2, DP // 2
    piece, depth, band = up_rows // UP, H // DP, own_rows // TP
    chunks = n * DC

    is_outer = (z == 0) | (z == n - 1)
    outer = jnp.where(z < n // 2, 0, n - 1)
    inner = jnp.where(z < n // 2, n // 2 - 1, n // 2)
    mate = n - 1 - inner
    far = n - 1 - outer
    unit = {"inner": inner, "mate": mate, "outer": outer, "far": far}

    def at(yy, zz, tt):
        return {"rep": yy, "fs": zz, "tp": tt}

    PARTNER = at(y, z, x * 2 + (1 - core))
    ASIDE = at(y, z, (1 - x) * 2 + core)
    ACROSS = at(1 - y, z, t)
    MATE = at(y, mate, t)
    OUTER = at(y, outer, t)
    INNER = at(y, inner, t)

    def remote(src, dst, send, recv, where):
        return pltpu.make_async_remote_copy(
            src_ref=src, dst_ref=dst, send_sem=send, recv_sem=recv,
            device_id=where, device_id_type=pl.DeviceIdType.MESH,
        )

    def up_slot(s, p):
        return upw.at[pl.ds(pl.multiple_of(s * up_rows + p * piece, piece), piece), :]

    def up_own(p):
        return up_hbm.at[pl.ds(pl.multiple_of(p * piece, piece), piece), :]

    def dn_slot(s, j, k):
        return dnw.at[s * DC + j, pl.ds(pl.multiple_of(k * depth, depth), depth), :]

    def dn_own(j, k):
        return dn_hbm.at[pl.ds(pl.multiple_of(k * depth, depth), depth), pl.ds(j * CW, CW)]

    def up_copy(s, p, src, where, other=False):
        slot = up_slot(s, p + ((1 - y) if other else y) * UM)
        crossing = where is ACROSS or other
        recv = up_recv.at[n * UM + s] if crossing else up_recv.at[s * UM + p]
        return remote(slot if src is None else src, slot, up_send.at[0], recv, where)

    def dn_copy(s, j, k, src, where, other=False):
        slot = dn_slot(s, j, k + ((1 - y) if other else y) * DM)
        crossing = where is ACROSS or other
        recv = dn_recv.at[chunks * DM + s * DC + j] if crossing else dn_recv.at[(s * DC + j) * DM + k]
        return remote(slot if src is None else src, slot, dn_send.at[0], recv, where)

    def up_landed(s, p):
        up_copy(s, p, None, MATE).wait_recv()

    def up_others(s):
        half = up_rows // 2
        ref = upw.at[pl.ds(pl.multiple_of(s * up_rows + (1 - y) * half, half), half), :]
        remote(ref, ref, up_send.at[0], up_recv.at[n * UM + s], MATE).wait_recv()

    def dn_landed(s, j, k):
        dn_copy(s, j, k, None, MATE).wait_recv()

    def dn_others(s, j):
        half = H // 2
        ref = dnw.at[s * DC + j, pl.ds(pl.multiple_of((1 - y) * half, half), half), :]
        remote(ref, ref, dn_send.at[0], dn_recv.at[chunks * DM + s * DC + j], MATE).wait_recv()

    def tok_slot(q, b):
        return tok.at[1, pl.ds(pl.multiple_of(q * own_rows + b * band, band), band), :]

    def tok_copy(recv, q, b, src, where):
        return remote(src, tok_slot(q, b), t_send.at[0], t_recv.at[recv], where)

    def tok_all(recv, q):
        ref = tok.at[1, pl.ds(pl.multiple_of(q * own_rows, own_rows), own_rows), :]
        remote(ref, ref, t_send.at[0], t_recv.at[recv], MATE).wait_recv()

    def sent(ref, sem, where):
        remote(ref, ref, sem.at[0], sem.at[0], where).wait_send()

    def out_cols(q):
        return out_hbm.at[:, pl.ds(pl.multiple_of(q * CW, CW), CW)]

    def column(i):
        return unit[ORDER[i][0]] * DC + ORDER[i][1]

    def own_copy(i):
        q = column(i)
        return pltpu.make_async_copy(outv.at[0, q], out_cols(q), own_sem.at[0])

    def own_done(count):
        width = pl.ds(0, count * CW)
        pltpu.make_async_copy(tok.at[0, pl.ds(0, own_rows), width], out_hbm.at[:, width], own_sem.at[0]).wait()

    def out_copy(i):
        q = column(i)
        return remote(outv.at[1, q], out_cols(q), o_send.at[0], o_recv.at[i], OUTER)

    def d_copy(i, to, of):
        return remote(dsend.at[i, to], drecv.at[i, of], d_send.at[0], d_recv.at[i], at(y, outer, to * 2 + core))

    def d_landed(i):
        remote(dsend.at[i], drecv.at[i], d_send.at[0], d_recv.at[i], INNER).wait_recv()

    barrier = pltpu.get_barrier_semaphore()

    def greet(peers):
        for peer in peers:
            pl.semaphore_signal(barrier, inc=1, device_id=peer, device_id_type=pl.DeviceIdType.MESH)

    mine_up, other_up = y * UM, (1 - y) * UM
    mine_dn, other_dn = y * DM, (1 - y) * DM
    passed = len(DIRECT)
    own_block = pl.ds(pl.multiple_of(t * own_rows, own_rows), own_rows)

    def own_tokens(src, q):
        return tok[src, own_block, pl.ds(pl.multiple_of(q * CW, CW), CW)].astype(jnp.float32)

    @pl.when(is_outer)
    def _():
        greet([INNER, at(y, inner, (1 - x) * 2 + core)])
        load = pltpu.make_async_copy(tok_hbm.at[own_block, :], tok.at[0, own_block, :], local.at[0])
        load.start()
        up_load = pltpu.make_async_copy(
            up_hbm, upw.at[pl.ds(pl.multiple_of(z * up_rows, up_rows), up_rows), :], local.at[2]
        )
        up_load.start()
        pl.semaphore_wait(barrier, 2)
        up_load.wait()
        for p in range(UM):
            up_copy(z, p, None, INNER).start()
        for b in range(TP):
            own = tok_hbm.at[pl.ds(pl.multiple_of(t * own_rows + b * band, band), band), :]
            tok_copy(b, t, b, own, INNER).start()
        for p in range(UM - BESIDE):
            up_copy(z, p, None, INNER, True).start()
        for j in range(DC):
            for k in range(DM):
                dn_copy(z, j, k, dn_own(j, mine_dn + k), INNER).start()
        for j in range(DC):
            for k in range(DM):
                dn_copy(z, j, k, dn_own(j, other_dn + k), INNER, True).start()
        load.wait()
        for i in range(chunks):
            if i in DIRECT:
                d_landed(i)
                q = column(i)
                res = own_tokens(0, q) + drecv[i, 0].astype(jnp.float32) + drecv[i, 1].astype(jnp.float32)
                outv[0, q] = res.astype(jnp.bfloat16)
                own_copy(i).start()
            else:
                out_copy(i).wait_recv()
        sent(upw.at[pl.ds(0, (2 * UM - BESIDE) * piece), :], up_send, INNER)
        sent(dnw.at[pl.ds(0, DC)], dn_send, INNER)
        sent(tok.at[0, pl.ds(0, own_rows), :], t_send, INNER)
        own_done(passed)

    @pl.when(jnp.logical_not(is_outer))
    def _():
        greet([PARTNER, ASIDE, ACROSS, MATE, OUTER, at(y, outer, (1 - x) * 2 + core)])
        tok_load = pltpu.make_async_copy(tok_hbm, tok.at[0], local.at[0])
        gain_load = pltpu.make_async_copy(gain_hbm, gain_ref, local.at[1])
        up_load = pltpu.make_async_copy(
            up_hbm, upw.at[pl.ds(pl.multiple_of(z * up_rows, up_rows), up_rows), :], local.at[2]
        )
        dn_loads = [
            pltpu.make_async_copy(dn_hbm.at[:, pl.ds(j * CW, CW)], dnw.at[z * DC + j], local.at[3 + j])
            for j in range(DC)
        ]
        for load in [up_load, gain_load, tok_load] + dn_loads:
            load.start()
        pl.semaphore_wait(barrier, 6)

        up_load.wait()
        for p in range(UM):
            up_copy(z, p, None, MATE).start()

        gain_load.wait()
        gain = gain_ref[...]

        def normalise(src, q):
            xf = tok[src, pl.ds(pl.multiple_of(q * own_rows, own_rows), own_rows), :].astype(jnp.float32)
            scale = lax.rsqrt(jnp.mean(xf * xf, axis=-1, keepdims=True) + EPS)
            to = (q % 2 * 2 + q // 2) * own_rows
            nrm[src, pl.ds(pl.multiple_of(to, own_rows), own_rows), :] = (xf * scale * gain).astype(jnp.bfloat16)

        def lift(src, start, size, first=False, last=False):
            k = pl.ds(pl.multiple_of(start, size), size)
            value = jnp.dot(nrm[src, :, k], upw[k, :], preferred_element_type=jnp.float32)
            if not first:
                value = value + lifted[src]
            if last:
                hid[src] = jnp.square(jnp.maximum(value, 0.0)).astype(jnp.bfloat16).reshape(2, rows // 2, H)
            else:
                lifted[src] = value

        def lift_mine(s):
            lift(0, s * up_rows + y * (up_rows // 2), up_rows // 2)

        def lift_others(s, last=False):
            up_others(s)
            lift(0, s * up_rows + (1 - y) * (up_rows // 2), up_rows // 2, last=last)

        def relay(name, j, k):
            s = unit[name]
            dn_landed(s, j, k)
            dn_copy(s, j, k, None, MATE if name == "outer" else ACROSS).start()

        def relay_up(s, p, where):
            up_copy(s, p, None, where).start()

        tok_load.wait()
        lax.fori_loop(0, 4, lambda q, carry: (normalise(0, q), carry)[1], 0)

        for p in range(UM):
            up_landed(outer, p)
            relay_up(outer, p, MATE)
            up_landed(mate, p)
            if p < UM - VIA_MATE:
                relay_up(mate, p, ACROSS)
            if p >= UM - BESIDE:
                relay_up(outer, p, ACROSS)
            if p == 1:
                lift(0, z * up_rows, up_rows, first=True)
        for p in range(UM - VIA_MATE, UM):
            up_copy(z, p, None, MATE, True).start()
        for j in range(DC):
            dn_loads[j].wait()
            for k in range(DM):
                dn_copy(z, j, k, dn_own(j, mine_dn + k), MATE).start()
        lift_mine(outer)
        lift_mine(mate)

        beside, beyond = x * 2 + 1 - core, (1 - x) * 2 + core
        corner = (1 - x) * 2 + 1 - core

        def pass_beyond(b):
            tok_copy(TP + b, beyond, b, tok_slot(beyond, b), ASIDE).wait_recv()
            tok_copy(2 * TP + 1, beyond, b, tok_slot(beyond, b), PARTNER).start()

        for b in range(TP):
            for p in range(b * UM // TP, (b + 1) * UM // TP):
                up_landed(far, p)
                relay_up(far, p, ACROSS)
            tok_copy(b, t, b, tok_slot(t, b), INNER).wait_recv()
            tok_copy(TP + b, t, b, tok_slot(t, b), ASIDE).start()
            tok_copy(2 * TP, t, b, tok_slot(t, b), PARTNER).start()
            if b > 1:
                pass_beyond(b - 2)
        normalise(1, t)
        lift_mine(far)
        tok_all(2 * TP, beside)
        normalise(1, beside)
        pass_beyond(TP - 2)
        pass_beyond(TP - 1)
        normalise(1, beyond)
        tok_all(2 * TP + 1, corner)
        normalise(1, corner)
        due = []
        for name, first in (("mate", 32.0), ("outer", 34.0), ("far", 44.0)):
            due += [(first + 1.4 * q, name, q // DM, q % DM) for q in range(DC * DM)]
        due.sort()

        def relays(until):
            while due and due[0][0] <= until:
                relay(*due.pop(0)[1:])

        relays(33)
        near = jnp.where(z < n // 2, 0, n // 2) * up_rows
        lift_others(outer)
        relays(34.5)
        lift(1, near, 2 * up_rows, first=True)
        relays(35.8)
        lift_others(mate)
        lift_others(far, last=True)

        def a_copy(i, src):
            return remote(asend.at[i, src], arecv.at[i, src], a_send.at[0], a_recv.at[i, src], PARTNER)

        def b_copy(i, src):
            return remote(bsend.at[i, src], brecv.at[i, src], b_send.at[0], b_recv.at[i, src], ASIDE)

        joining, finishing = [], []

        def join(left=0):
            while len(joining) > left:
                i, src = joining.pop(0)
                a_copy(i, src).wait_recv()

                def added(to):
                    return part[i % 2, src, core, to] + arecv[i, src, to].astype(jnp.float32)

                if src == 1 and i in DIRECT:
                    for to in (0, 1):
                        dsend[i, to] = added(to).astype(jnp.bfloat16)
                        d_copy(i, to, x).start()
                else:
                    bsend[i, src] = added(1 - x).astype(jnp.bfloat16)
                    b_copy(i, src).start()
                    keep[i, src] = added(x)
                    finishing.append((i, src))

        def finish(left):
            while len(finishing) > left:
                i, src = finishing.pop(0)
                q = column(i)
                b_copy(i, src).wait_recv()
                res = own_tokens(src, q) + keep[i, src] + brecv[i, src].astype(jnp.float32)
                outv[src, q] = res.astype(jnp.bfloat16)
                (own_copy if src == 0 else out_copy)(i).start()

        def give(i, src):
            asend[i, src] = part[i % 2, src, 1 - core].astype(jnp.bfloat16)
            a_copy(i, src).start()

        def compute(i, src):
            product = jnp.dot(hid[src].reshape(rows, H), dnw[column(i)], preferred_element_type=jnp.float32)
            part[i % 2, src] = product.reshape(2, 2, own_rows, CW)
            give(i, src)
            join()
            joining.append((i, src))
            finish(LAG)

        def both(i):
            name, j = ORDER[i]
            if name != "inner":
                dn_others(unit[name], j)
            product = jnp.dot(hid[...].reshape(2 * rows, H), dnw[column(i)], preferred_element_type=jnp.float32)
            part[i % 2] = product.reshape(2, 2, 2, own_rows, CW)
            give(i, 1)
            give(i, 0)
            join()
            joining.extend([(i, 1), (i, 0)])
            finish(LAG)

        relays(37)
        compute(0, 0)
        compute(1, 0)
        relays(38)
        lift(1, (n // 2) * up_rows - near, 2 * up_rows, last=True)
        join()
        relays(39.5)
        compute(0, 1)
        relays(40.5)
        compute(1, 1)
        relays(41.5)
        join()
        relays(43)
        both(2)
        relays(44.5)
        join()
        relays(46)
        both(3)
        relays(47.5)
        join()
        relays(50)
        both(4)
        relays(51.5)
        join()
        relays(52.5)
        both(5)
        relays(54)
        join()
        relays(99)
        both(6)
        both(7)
        join()
        finish(0)

        ups = 2 * UM + VIA_MATE + (UM - VIA_MATE) + UM + BESIDE
        sent(upw.at[pl.ds(0, ups * piece), :], up_send, MATE)
        sent(dnw.at[pl.ds(0, 2 * DC)], dn_send, MATE)
        sent(tok.at[0, pl.ds(0, 3 * own_rows), :], t_send, MATE)
        sent(asend, a_send, PARTNER)
        sent(bsend.at[pl.ds(0, chunks - passed // 2)], b_send, ASIDE)
        sent(outv.at[1, pl.ds(0, chunks - passed)], o_send, OUTER)
        sent(dsend.at[pl.ds(0, passed)], d_send, OUTER)
        own_done(chunks)


def fused(n, tokens, norm_gain, up_weight, down_weight):
    rows, D = tokens.shape
    up_rows, H = up_weight.shape
    CW = down_weight.shape[1] // DN_CHUNKS
    chunks = n * DN_CHUNKS
    own_rows = rows // 4
    bf, f32 = jnp.bfloat16, jnp.float32
    dma = pltpu.SemaphoreType.DMA
    return pl.pallas_call(
        functools.partial(kernel, n),
        out_shape=jax.ShapeDtypeStruct((own_rows, D), bf),
        in_specs=[pl.BlockSpec(memory_space=pl.ANY)] * 4,
        out_specs=pl.BlockSpec(memory_space=pl.ANY),
        scratch_shapes=[
            pltpu.VMEM((1, D), f32),
            pltpu.VMEM((2, rows, D), bf),
            pltpu.VMEM((2, rows, D), bf),
            pltpu.VMEM((n * up_rows, H), bf),
            pltpu.VMEM((chunks, H, CW), bf),
            pltpu.VMEM((2, rows, H), f32),
            pltpu.VMEM((2, 2, rows // 2, H), bf),
            pltpu.VMEM((2, 2, 2, 2, own_rows, CW), f32),
            pltpu.VMEM((chunks, 2, 2, own_rows, CW), bf),
            pltpu.VMEM((chunks, 2, 2, own_rows, CW), bf),
            pltpu.VMEM((chunks, 2, own_rows, CW), bf),
            pltpu.VMEM((chunks, 2, own_rows, CW), bf),
            pltpu.VMEM((chunks, 2, own_rows, CW), f32),
            pltpu.VMEM((2, chunks, own_rows, CW), bf),
            pltpu.VMEM((chunks, 2, own_rows, CW), bf),
            pltpu.VMEM((chunks, 2, own_rows, CW), bf),
            dma((1,)),
            dma((n * (UP_PIECES // 2 + 1),)),
            dma((1,)),
            dma((chunks * (DN_PIECES // 2 + 1),)),
            dma((1,)),
            dma((2 * TOK_PIECES + 2,)),
            dma((1,)),
            dma((chunks, 2)),
            dma((1,)),
            dma((chunks, 2)),
            dma((1,)),
            dma((chunks,)),
            dma((1,)),
            dma((chunks,)),
            dma((1,)),
            dma((3 + DN_CHUNKS,)),
        ],
        compiler_params=pltpu.CompilerParams(
            collective_id=0, has_side_effects=True, vmem_limit_bytes=53 * 1024 * 1024
        ),
    )(tokens, norm_gain.reshape(1, D), up_weight, down_weight)


def fits(mesh, tokens, up_weight, down_weight):
    n = mesh.shape["fs"]
    rows = tokens.shape[0] // (mesh.shape["rep"] * n)
    columns = down_weight.shape[1] // n
    depth = up_weight.shape[0] // n
    hidden = up_weight.shape[1] // mesh.shape["tp"]
    return (
        mesh.shape["rep"] == 2
        and mesh.shape["tp"] == 4
        and n == 4
        and columns % (128 * DN_CHUNKS) == 0
        and depth % (UP_PIECES * 16) == 0
        and depth % 128 == 0
        and hidden % (16 * DN_PIECES) == 0
        and hidden % 128 == 0
        and rows % (4 * 16 * TOK_PIECES) == 0
        and rows <= 512
        and hidden <= 1024
        and tokens.shape[1] <= 2048
    )


def solution(mesh):
    placed = (P(("rep", "fs"), None), P(), P("fs", "tp"), P("tp", "fs"))

    def layer(tokens, norm_gain, up_weight, down_weight):
        if fits(mesh, tokens, up_weight, down_weight):
            body = functools.partial(fused, mesh.shape["fs"])
        else:
            body = shards
        return jax.shard_map(
            body, mesh=mesh, in_specs=placed, out_specs=P(("rep", "fs", "tp"), None), check_vma=False
        )(tokens, norm_gain, up_weight, down_weight)

    return layer
```

```python
import functools

import jax
import jax.numpy as jnp
from jax import lax
from jax.experimental import pallas as pl
from jax.experimental.pallas import tpu as pltpu
from jax.sharding import PartitionSpec as P

EPS = 1e-06
UP_PIECES = 16
DN_CHUNKS = 2
DN_PIECES = 8
TOK_PIECES = 4
BESIDE = 4
VIA_MATE = 2
LAG = 4
ORDER = (
    ("inner", 0), ("inner", 1), ("mate", 0), ("mate", 1),
    ("outer", 0), ("far", 0), ("outer", 1), ("far", 1),
)
DIRECT = (1, 4, 5, 7)


def shards(tokens, norm_gain, up_weight, down_weight):
    xf = tokens.astype(jnp.float32)
    scale = lax.rsqrt(jnp.mean(xf * xf, axis=-1, keepdims=True) + EPS)
    normed = (xf * scale * norm_gain).astype(jnp.bfloat16)
    rows = tokens.shape[0]
    halves = lax.axis_size("rep")
    share = up_weight.shape[0] // halves
    mine = lax.dynamic_slice_in_dim(up_weight, lax.axis_index("rep") * share, share, 0)
    arranged = normed.reshape(rows, -1, halves, share).transpose(0, 2, 1, 3).reshape(rows, -1)
    lifted = jnp.dot(
        arranged,
        lax.all_gather(mine, ("rep", "fs"), axis=0, tiled=True),
        preferred_element_type=jnp.float32,
    )
    width = down_weight.shape[1] // halves
    down_mine = lax.dynamic_slice_in_dim(down_weight, lax.axis_index("rep") * width, width, 1)
    collected = lax.all_gather(down_mine, ("rep", "fs"), axis=1, tiled=True)
    hidden_rows = collected.shape[0]
    down_block = (
        collected.reshape(hidden_rows, halves, -1, width)
        .transpose(0, 2, 1, 3)
        .reshape(hidden_rows, -1)
    )
    hidden = jnp.square(jnp.maximum(lifted, 0.0)).astype(jnp.bfloat16)
    own_rows = rows // lax.axis_size("tp")
    summed = lax.psum_scatter(
        jnp.dot(hidden, down_block, preferred_element_type=jnp.float32).astype(jnp.bfloat16),
        "tp",
        scatter_dimension=0,
        tiled=True,
    ).astype(jnp.float32)
    residual = lax.dynamic_slice_in_dim(xf, lax.axis_index("tp") * own_rows, own_rows, 0)
    return (residual + summed).astype(jnp.bfloat16)


def kernel(
    n, tok_hbm, gain_hbm, up_hbm, dn_hbm, out_hbm,
    gain_ref, tok, nrm, upw, dnw, lifted, hid, part, asend, arecv, bsend, brecv, keep, outv, dsend, drecv,
    up_send, up_recv, dn_send, dn_recv, t_send, t_recv,
    a_send, a_recv, b_send, b_recv, o_send, o_recv, d_send, d_recv, own_sem, local,
):
    y, z, t = lax.axis_index("rep"), lax.axis_index("fs"), lax.axis_index("tp")
    x, core = t // 2, t % 2
    rows = tok_hbm.shape[0]
    own_rows = rows // 4
    up_rows, H = up_hbm.shape
    CW = dnw.shape[2]
    UP, DC, DP, TP = UP_PIECES, DN_CHUNKS, DN_PIECES, TOK_PIECES
    UM, DM = UP // 2, DP // 2
    piece, depth, band = up_rows // UP, H // DP, own_rows // TP
    chunks = n * DC
    HALF = CW // 2

    is_outer = (z == 0) | (z == n - 1)
    outer = jnp.where(z < n // 2, 0, n - 1)
    inner = jnp.where(z < n // 2, n // 2 - 1, n // 2)
    mate = n - 1 - inner
    far = n - 1 - outer
    unit = {"inner": inner, "mate": mate, "outer": outer, "far": far}

    def at(yy, zz, tt):
        return {"rep": yy, "fs": zz, "tp": tt}

    PARTNER = at(y, z, x * 2 + (1 - core))
    ASIDE = at(y, z, (1 - x) * 2 + core)
    ACROSS = at(1 - y, z, t)
    MATE = at(y, mate, t)
    OUTER = at(y, outer, t)
    INNER = at(y, inner, t)

    def remote(src, dst, send, recv, where):
        return pltpu.make_async_remote_copy(
            src_ref=src, dst_ref=dst, send_sem=send, recv_sem=recv,
            device_id=where, device_id_type=pl.DeviceIdType.MESH,
        )

    def up_slot(s, p):
        return upw.at[pl.ds(pl.multiple_of(s * up_rows + p * piece, piece), piece), :]

    def up_own(p):
        return up_hbm.at[pl.ds(pl.multiple_of(p * piece, piece), piece), :]

    def dn_part(j, k, other):
        side = ((1 - y) if other else y) * (H // 2)
        if j < DC - 1:
            return pl.ds(pl.multiple_of(side + k * depth, depth), depth), pl.ds(0, CW)
        return pl.ds(pl.multiple_of(side + k % 2 * 2 * depth, 2 * depth), 2 * depth), pl.ds(k // 2 * HALF, HALF)

    def dn_slot(s, j, k, other=False):
        r, c = dn_part(j, k, other)
        return dnw.at[s * DC + j, r, c]

    def dn_own(j, k, other=False):
        r, c = dn_part(j, k, other)
        return dn_hbm.at[r, pl.ds(j * CW + c.start, c.size)]

    def up_copy(s, p, src, where, other=False):
        slot = up_slot(s, p + ((1 - y) if other else y) * UM)
        crossing = where is ACROSS or other
        recv = up_recv.at[n * UM + s] if crossing else up_recv.at[s * UM + p]
        return remote(slot if src is None else src, slot, up_send.at[0], recv, where)

    def dn_copy(s, j, k, where, other=False, stored=False):
        slot = dn_slot(s, j, k, other)
        if where is ACROSS or other:
            recv = dn_recv.at[chunks * DM + s * (DC + 1) + j + (k // 2 if j == DC - 1 else 0)]
        else:
            recv = dn_recv.at[(s * DC + j) * DM + k]
        return remote(dn_own(j, k, other) if stored else slot, slot, dn_send.at[0], recv, where)

    def up_landed(s, p):
        up_copy(s, p, None, MATE).wait_recv()

    def up_others(s):
        half = up_rows // 2
        ref = upw.at[pl.ds(pl.multiple_of(s * up_rows + (1 - y) * half, half), half), :]
        remote(ref, ref, up_send.at[0], up_recv.at[n * UM + s], MATE).wait_recv()

    def dn_landed(s, j, k):
        dn_copy(s, j, k, MATE).wait_recv()

    def dn_others(s, j, h=0):
        cols = pl.ds(h * HALF, HALF) if j == DC - 1 else pl.ds(0, CW)
        ref = dnw.at[s * DC + j, pl.ds(pl.multiple_of((1 - y) * (H // 2), H // 2), H // 2), cols]
        remote(ref, ref, dn_send.at[0], dn_recv.at[chunks * DM + s * (DC + 1) + j + h], MATE).wait_recv()

    def tok_slot(q, b):
        return tok.at[1, pl.ds(pl.multiple_of(q * own_rows + b * band, band), band), :]

    def tok_copy(recv, q, b, src, where):
        return remote(src, tok_slot(q, b), t_send.at[0], t_recv.at[recv], where)

    def tok_all(recv, q):
        ref = tok.at[1, pl.ds(pl.multiple_of(q * own_rows, own_rows), own_rows), :]
        remote(ref, ref, t_send.at[0], t_recv.at[recv], MATE).wait_recv()

    def sent(ref, sem, where):
        remote(ref, ref, sem.at[0], sem.at[0], where).wait_send()

    def column(i):
        return unit[ORDER[i][0]] * DC + ORDER[i][1]

    def cut(h):
        return pl.ds(0, CW) if h is None else pl.ds(h * HALF, HALF)

    def mark(i, h):
        return chunks if h == 1 else i

    def out_part(q, h):
        start = pl.multiple_of(q * CW + (h or 0) * HALF, HALF)
        return out_hbm.at[:, pl.ds(start, CW if h is None else HALF)]

    def own_copy(i, h=None):
        q = column(i)
        return pltpu.make_async_copy(outv.at[0, q, :, cut(h)], out_part(q, h), own_sem.at[0])

    def own_done(count):
        width = pl.ds(0, count * CW)
        pltpu.make_async_copy(tok.at[0, pl.ds(0, own_rows), width], out_hbm.at[:, width], own_sem.at[0]).wait()

    def out_copy(i, h=None):
        q = column(i)
        return remote(outv.at[1, q, :, cut(h)], out_part(q, h), o_send.at[0], o_recv.at[mark(i, h)], OUTER)

    def d_copy(i, to, of, h=None):
        return remote(dsend.at[i, to, :, cut(h)], drecv.at[i, of, :, cut(h)], d_send.at[0], d_recv.at[mark(i, h)],
                      at(y, outer, to * 2 + core))

    def d_landed(i, h=None):
        ref = drecv.at[i, :, :, cut(h)]
        remote(ref, ref, d_send.at[0], d_recv.at[mark(i, h)], INNER).wait_recv()

    barrier = pltpu.get_barrier_semaphore()

    def greet(peers):
        for peer in peers:
            pl.semaphore_signal(barrier, inc=1, device_id=peer, device_id_type=pl.DeviceIdType.MESH)

    mine_up, other_up = y * UM, (1 - y) * UM
    passed = len(DIRECT)
    own_block = pl.ds(pl.multiple_of(t * own_rows, own_rows), own_rows)

    def own_tokens(src, q, h=None):
        start = pl.multiple_of(q * CW + (h or 0) * HALF, HALF)
        return tok[src, own_block, pl.ds(start, CW if h is None else HALF)].astype(jnp.float32)

    @pl.when(is_outer)
    def _():
        greet([INNER, at(y, inner, (1 - x) * 2 + core)])
        load = pltpu.make_async_copy(tok_hbm.at[own_block, :], tok.at[0, own_block, :], local.at[0])
        load.start()
        up_load = pltpu.make_async_copy(
            up_hbm, upw.at[pl.ds(pl.multiple_of(z * up_rows, up_rows), up_rows), :], local.at[2]
        )
        up_load.start()
        pl.semaphore_wait(barrier, 2)
        up_load.wait()
        for p in range(UM):
            up_copy(z, p, None, INNER).start()
        for b in range(TP):
            own = tok_hbm.at[pl.ds(pl.multiple_of(t * own_rows + b * band, band), band), :]
            tok_copy(b, t, b, own, INNER).start()
        for p in range(UM - BESIDE):
            up_copy(z, p, None, INNER, True).start()
        for other in (False, True):
            for j in range(DC):
                for k in range(DM):
                    dn_copy(z, j, k, INNER, other, True).start()
        load.wait()
        for i in range(chunks):
            for h in (0, 1) if i == chunks - 1 else (None,):
                if i in DIRECT:
                    d_landed(i, h)
                    q, c = column(i), cut(h)
                    res = own_tokens(0, q, h) + drecv[i, 0, :, c].astype(jnp.float32)
                    outv[0, q, :, c] = (res + drecv[i, 1, :, c].astype(jnp.float32)).astype(jnp.bfloat16)
                    own_copy(i, h).start()
                else:
                    out_copy(i, h).wait_recv()
        sent(upw.at[pl.ds(0, (2 * UM - BESIDE) * piece), :], up_send, INNER)
        sent(dnw.at[pl.ds(0, DC)], dn_send, INNER)
        sent(tok.at[0, pl.ds(0, own_rows), :], t_send, INNER)
        own_done(passed)

    @pl.when(jnp.logical_not(is_outer))
    def _():
        greet([PARTNER, ASIDE, ACROSS, MATE, OUTER, at(y, outer, (1 - x) * 2 + core)])
        tok_load = pltpu.make_async_copy(tok_hbm, tok.at[0], local.at[0])
        gain_load = pltpu.make_async_copy(gain_hbm, gain_ref, local.at[1])
        up_load = pltpu.make_async_copy(
            up_hbm, upw.at[pl.ds(pl.multiple_of(z * up_rows, up_rows), up_rows), :], local.at[2]
        )
        dn_loads = [
            pltpu.make_async_copy(dn_hbm.at[:, pl.ds(j * CW, CW)], dnw.at[z * DC + j], local.at[3 + j])
            for j in range(DC)
        ]
        for load in [up_load, gain_load, tok_load] + dn_loads:
            load.start()
        pl.semaphore_wait(barrier, 6)

        up_load.wait()
        for p in range(UM):
            up_copy(z, p, None, MATE).start()

        gain_load.wait()
        gain = gain_ref[...]

        def normalise(src, q):
            xf = tok[src, pl.ds(pl.multiple_of(q * own_rows, own_rows), own_rows), :].astype(jnp.float32)
            scale = lax.rsqrt(jnp.mean(xf * xf, axis=-1, keepdims=True) + EPS)
            to = (q % 2 * 2 + q // 2) * own_rows
            nrm[src, pl.ds(pl.multiple_of(to, own_rows), own_rows), :] = (xf * scale * gain).astype(jnp.bfloat16)

        def lift(src, start, size, first=False, last=False):
            k = pl.ds(pl.multiple_of(start, size), size)
            value = jnp.dot(nrm[src, :, k], upw[k, :], preferred_element_type=jnp.float32)
            if not first:
                value = value + lifted[src]
            if last:
                hid[src] = jnp.square(jnp.maximum(value, 0.0)).astype(jnp.bfloat16).reshape(2, rows // 2, H)
            else:
                lifted[src] = value

        def lift_mine(s):
            lift(0, s * up_rows + y * (up_rows // 2), up_rows // 2)

        def lift_others(s, last=False):
            up_others(s)
            lift(0, s * up_rows + (1 - y) * (up_rows // 2), up_rows // 2, last=last)

        def relay(name, j, k):
            s = unit[name]
            dn_landed(s, j, k)
            dn_copy(s, j, k, MATE if name == "outer" else ACROSS).start()

        def relay_up(s, p, where):
            up_copy(s, p, None, where).start()

        tok_load.wait()
        lax.fori_loop(0, 4, lambda q, carry: (normalise(0, q), carry)[1], 0)

        for p in range(UM):
            up_landed(outer, p)
            relay_up(outer, p, MATE)
            up_landed(mate, p)
            if p < UM - VIA_MATE:
                relay_up(mate, p, ACROSS)
            if p >= UM - BESIDE:
                relay_up(outer, p, ACROSS)
            if p == 1:
                lift(0, z * up_rows, up_rows, first=True)
        for p in range(UM - VIA_MATE, UM):
            up_copy(z, p, None, MATE, True).start()
        for j in range(DC):
            dn_loads[j].wait()
            for k in range(DM):
                dn_copy(z, j, k, MATE, False, True).start()
        lift_mine(outer)
        lift_mine(mate)

        beside, beyond = x * 2 + 1 - core, (1 - x) * 2 + core
        corner = (1 - x) * 2 + 1 - core

        def pass_beyond(b):
            tok_copy(TP + b, beyond, b, tok_slot(beyond, b), ASIDE).wait_recv()
            tok_copy(2 * TP + 1, beyond, b, tok_slot(beyond, b), PARTNER).start()

        for b in range(TP):
            for p in range(b * UM // TP, (b + 1) * UM // TP):
                up_landed(far, p)
                relay_up(far, p, ACROSS)
            tok_copy(b, t, b, tok_slot(t, b), INNER).wait_recv()
            tok_copy(TP + b, t, b, tok_slot(t, b), ASIDE).start()
            tok_copy(2 * TP, t, b, tok_slot(t, b), PARTNER).start()
            if b > 1:
                pass_beyond(b - 2)
        due = []
        for name, first in (("mate", 32.2), ("outer", 34.0), ("far", 43.5)):
            due += [(first + 1.4 * q, name, q // DM, q % DM) for q in range(DC * DM)]
        due.sort()

        def relays(until):
            while due and due[0][0] <= until:
                relay(*due.pop(0)[1:])

        normalise(1, t)
        lift_mine(far)
        tok_all(2 * TP, beside)
        normalise(1, beside)
        pass_beyond(TP - 2)
        pass_beyond(TP - 1)
        normalise(1, beyond)
        relays(33)
        tok_all(2 * TP + 1, corner)
        normalise(1, corner)
        near = jnp.where(z < n // 2, 0, n // 2) * up_rows
        lift_others(outer)
        relays(33.7)
        lift(1, near, 2 * up_rows, first=True)
        relays(35)
        lift_others(mate)
        relays(35.5)
        lift_others(far, last=True)
        relays(36.5)
        lift(1, (n // 2) * up_rows - near, 2 * up_rows, last=True)
        relays(37.8)

        def a_copy(i, src, h=None):
            return remote(asend.at[i, src, :, :, cut(h)], arecv.at[i, src, :, :, cut(h)],
                          a_send.at[0], a_recv.at[mark(i, h), src], PARTNER)

        def b_copy(i, src, h=None):
            return remote(bsend.at[i, src, :, cut(h)], brecv.at[i, src, :, cut(h)],
                          b_send.at[0], b_recv.at[mark(i, h), src], ASIDE)

        joining, finishing = [], []

        def join(left=0):
            while len(joining) > left:
                i, src, h = joining.pop(0)
                c = cut(h)
                a_copy(i, src, h).wait_recv()

                def added(to):
                    return part[i % 2, src, core, to, :, c] + arecv[i, src, to, :, c].astype(jnp.float32)

                if src == 1 and i in DIRECT:
                    for to in (1 - x, x):
                        dsend[i, to, :, c] = added(to).astype(jnp.bfloat16)
                        d_copy(i, to, x, h).start()
                else:
                    bsend[i, src, :, c] = added(1 - x).astype(jnp.bfloat16)
                    b_copy(i, src, h).start()
                    keep[i, src, :, c] = added(x)
                    finishing.append((i, src, h))

        def pick(*item):
            joining.remove(item)
            joining.insert(0, item)
            join(len(joining) - 1)

        def finish(left):
            while len(finishing) > left:
                i, src, h = finishing.pop(0)
                q, c = column(i), cut(h)
                b_copy(i, src, h).wait_recv()
                res = own_tokens(src, q, h) + keep[i, src, :, c] + brecv[i, src, :, c].astype(jnp.float32)
                outv[src, q, :, c] = res.astype(jnp.bfloat16)
                (own_copy if src == 0 else out_copy)(i, h).start()

        def give(i, src, h=None):
            c = cut(h)
            asend[i, src, :, :, c] = part[i % 2, src, 1 - core, :, :, c].astype(jnp.bfloat16)
            a_copy(i, src, h).start()
            joining.append((i, src, h))

        def arrive(i):
            name, j = ORDER[i]
            if name != "inner":
                for h in (0, 1) if j == DC - 1 else (0,):
                    dn_others(unit[name], j, h)

        def compute(i, src, h=None):
            block = dnw[column(i), :, cut(h)]
            for side in (0, 1):
                product = jnp.dot(hid[src, side], block, preferred_element_type=jnp.float32)
                part[i % 2, src, side, :, :, cut(h)] = product.reshape(2, own_rows, block.shape[1])
            give(i, src, h)

        def both(i, h=None):
            block = dnw[column(i), :, cut(h)]
            for src in (0, 1):
                product = jnp.dot(hid[src].reshape(rows, H), block, preferred_element_type=jnp.float32)
                part[i % 2, src, :, :, :, cut(h)] = product.reshape(2, 2, own_rows, block.shape[1])
            give(i, 1, h)
            give(i, 0, h)

        both(0)
        relays(39.2)
        both(1)
        join(2)
        relays(40.6)
        join()
        relays(42)
        arrive(2)
        both(2)
        relays(43.6)
        join()
        relays(46.4)
        finish(3)
        arrive(3)
        both(3)
        relays(47.8)
        finish(2)
        join()
        relays(49.2)
        finish(2)
        arrive(4)
        both(4)
        relays(50.6)
        join()
        relays(52)
        relays(99)
        arrive(5)
        both(5)
        finish(1)
        arrive(6)
        compute(6, 1)
        join(1)
        compute(6, 0)
        finish(2)
        dn_others(far, DC - 1, 0)
        both(7, 0)
        pick(6, 1, None)
        dn_others(far, DC - 1, 1)
        compute(7, 1, 1)
        pick(7, 1, 0)
        compute(7, 0, 1)
        pick(7, 1, 1)
        finish(0)
        join()
        finish(0)

        ups = 2 * UM + VIA_MATE + (UM - VIA_MATE) + UM + BESIDE
        sent(upw.at[pl.ds(0, ups * piece), :], up_send, MATE)
        sent(dnw.at[pl.ds(0, 2 * DC)], dn_send, MATE)
        sent(tok.at[0, pl.ds(0, 3 * own_rows), :], t_send, MATE)
        sent(asend, a_send, PARTNER)
        sent(bsend.at[pl.ds(0, chunks - passed // 2)], b_send, ASIDE)
        sent(outv.at[1, pl.ds(0, chunks - passed)], o_send, OUTER)
        sent(dsend.at[pl.ds(0, passed)], d_send, OUTER)
        own_done(chunks)


def fused(n, tokens, norm_gain, up_weight, down_weight):
    rows, D = tokens.shape
    up_rows, H = up_weight.shape
    CW = down_weight.shape[1] // DN_CHUNKS
    chunks = n * DN_CHUNKS
    own_rows = rows // 4
    bf, f32 = jnp.bfloat16, jnp.float32
    dma = pltpu.SemaphoreType.DMA
    return pl.pallas_call(
        functools.partial(kernel, n),
        out_shape=jax.ShapeDtypeStruct((own_rows, D), bf),
        in_specs=[pl.BlockSpec(memory_space=pl.ANY)] * 4,
        out_specs=pl.BlockSpec(memory_space=pl.ANY),
        scratch_shapes=[
            pltpu.VMEM((1, D), f32),
            pltpu.VMEM((2, rows, D), bf),
            pltpu.VMEM((2, rows, D), bf),
            pltpu.VMEM((n * up_rows, H), bf),
            pltpu.VMEM((chunks, H, CW), bf),
            pltpu.VMEM((2, rows, H), f32),
            pltpu.VMEM((2, 2, rows // 2, H), bf),
            pltpu.VMEM((2, 2, 2, 2, own_rows, CW), f32),
            pltpu.VMEM((chunks, 2, 2, own_rows, CW), bf),
            pltpu.VMEM((chunks, 2, 2, own_rows, CW), bf),
            pltpu.VMEM((chunks, 2, own_rows, CW), bf),
            pltpu.VMEM((chunks, 2, own_rows, CW), bf),
            pltpu.VMEM((chunks, 2, own_rows, CW), f32),
            pltpu.VMEM((2, chunks, own_rows, CW), bf),
            pltpu.VMEM((chunks, 2, own_rows, CW), bf),
            pltpu.VMEM((chunks, 2, own_rows, CW), bf),
            dma((1,)),
            dma((n * (UP_PIECES // 2 + 1),)),
            dma((1,)),
            dma((chunks * (DN_PIECES // 2 + 1) + n,)),
            dma((1,)),
            dma((2 * TOK_PIECES + 2,)),
            dma((1,)),
            dma((chunks + 1, 2)),
            dma((1,)),
            dma((chunks + 1, 2)),
            dma((1,)),
            dma((chunks + 1,)),
            dma((1,)),
            dma((chunks + 1,)),
            dma((1,)),
            dma((3 + DN_CHUNKS,)),
        ],
        compiler_params=pltpu.CompilerParams(
            collective_id=0, has_side_effects=True, vmem_limit_bytes=53 * 1024 * 1024
        ),
    )(tokens, norm_gain.reshape(1, D), up_weight, down_weight)


def fits(mesh, tokens, up_weight, down_weight):
    n = mesh.shape["fs"]
    rows = tokens.shape[0] // (mesh.shape["rep"] * n)
    columns = down_weight.shape[1] // n
    depth = up_weight.shape[0] // n
    hidden = up_weight.shape[1] // mesh.shape["tp"]
    return (
        mesh.shape["rep"] == 2
        and mesh.shape["tp"] == 4
        and n == 4
        and columns % (256 * DN_CHUNKS) == 0
        and depth % (UP_PIECES * 16) == 0
        and depth % 128 == 0
        and hidden % (16 * DN_PIECES) == 0
        and hidden % 128 == 0
        and rows % (4 * 16 * TOK_PIECES) == 0
        and rows <= 512
        and hidden <= 1024
        and tokens.shape[1] <= 2048
    )


def solution(mesh):
    placed = (P(("rep", "fs"), None), P(), P("fs", "tp"), P("tp", "fs"))

    def layer(tokens, norm_gain, up_weight, down_weight):
        if fits(mesh, tokens, up_weight, down_weight):
            body = functools.partial(fused, mesh.shape["fs"])
        else:
            body = shards
        return jax.shard_map(
            body, mesh=mesh, in_specs=placed, out_specs=P(("rep", "fs", "tp"), None), check_vma=False
        )(tokens, norm_gain, up_weight, down_weight)

    return layer
```

```python
import functools

import jax
import jax.numpy as jnp
from jax import lax
from jax.experimental import pallas as pl
from jax.experimental.pallas import tpu as pltpu
from jax.sharding import PartitionSpec as P

EPS = 1e-06
UP_PIECES = 16
DN_CHUNKS = 2
DN_PIECES = 8
TOK_PIECES = 4
BESIDE = 4
VIA_MATE = 2
LAG = 4
ORDER = (
    ("inner", 0), ("inner", 1), ("mate", 0), ("mate", 1),
    ("outer", 0), ("far", 0), ("outer", 1), ("far", 1),
)
DIRECT = (1, 2, 3, 4, 5, 7)


def shards(tokens, norm_gain, up_weight, down_weight):
    xf = tokens.astype(jnp.float32)
    scale = lax.rsqrt(jnp.mean(xf * xf, axis=-1, keepdims=True) + EPS)
    normed = (xf * scale * norm_gain).astype(jnp.bfloat16)
    rows = tokens.shape[0]
    halves = lax.axis_size("rep")
    share = up_weight.shape[0] // halves
    mine = lax.dynamic_slice_in_dim(up_weight, lax.axis_index("rep") * share, share, 0)
    arranged = normed.reshape(rows, -1, halves, share).transpose(0, 2, 1, 3).reshape(rows, -1)
    lifted = jnp.dot(
        arranged,
        lax.all_gather(mine, ("rep", "fs"), axis=0, tiled=True),
        preferred_element_type=jnp.float32,
    )
    width = down_weight.shape[1] // halves
    down_mine = lax.dynamic_slice_in_dim(down_weight, lax.axis_index("rep") * width, width, 1)
    collected = lax.all_gather(down_mine, ("rep", "fs"), axis=1, tiled=True)
    hidden_rows = collected.shape[0]
    down_block = (
        collected.reshape(hidden_rows, halves, -1, width)
        .transpose(0, 2, 1, 3)
        .reshape(hidden_rows, -1)
    )
    hidden = jnp.square(jnp.maximum(lifted, 0.0)).astype(jnp.bfloat16)
    own_rows = rows // lax.axis_size("tp")
    summed = lax.psum_scatter(
        jnp.dot(hidden, down_block, preferred_element_type=jnp.float32).astype(jnp.bfloat16),
        "tp",
        scatter_dimension=0,
        tiled=True,
    ).astype(jnp.float32)
    residual = lax.dynamic_slice_in_dim(xf, lax.axis_index("tp") * own_rows, own_rows, 0)
    return (residual + summed).astype(jnp.bfloat16)


def kernel(
    n, tok_hbm, gain_hbm, up_hbm, dn_hbm, out_hbm,
    gain_ref, tok, nrm, upw, dnw, lifted, hid, part, asend, arecv, bsend, brecv, keep, outv, dsend, drecv,
    up_send, up_recv, dn_send, dn_recv, t_send, t_recv,
    a_send, a_recv, b_send, b_recv, o_send, o_recv, d_send, own_sem, local,
):
    y, z, t = lax.axis_index("rep"), lax.axis_index("fs"), lax.axis_index("tp")
    x, core = t // 2, t % 2
    rows = tok_hbm.shape[0]
    own_rows = rows // 4
    up_rows, H = up_hbm.shape
    CW = dnw.shape[2]
    UP, DC, DP, TP = UP_PIECES, DN_CHUNKS, DN_PIECES, TOK_PIECES
    UM, DM = UP // 2, DP // 2
    piece, depth, band = up_rows // UP, H // DP, own_rows // TP
    chunks = n * DC
    HALF = CW // 2

    is_outer = (z == 0) | (z == n - 1)
    outer = jnp.where(z < n // 2, 0, n - 1)
    inner = jnp.where(z < n // 2, n // 2 - 1, n // 2)
    mate = n - 1 - inner
    far = n - 1 - outer
    unit = {"inner": inner, "mate": mate, "outer": outer, "far": far}

    def at(yy, zz, tt):
        return {"rep": yy, "fs": zz, "tp": tt}

    PARTNER = at(y, z, x * 2 + (1 - core))
    ASIDE = at(y, z, (1 - x) * 2 + core)
    ACROSS = at(1 - y, z, t)
    MATE = at(y, mate, t)
    OUTER = at(y, outer, t)
    INNER = at(y, inner, t)

    def remote(src, dst, send, recv, where):
        return pltpu.make_async_remote_copy(
            src_ref=src, dst_ref=dst, send_sem=send, recv_sem=recv,
            device_id=where, device_id_type=pl.DeviceIdType.MESH,
        )

    def up_slot(s, p):
        return upw.at[pl.ds(pl.multiple_of(s * up_rows + p * piece, piece), piece), :]

    def up_own(p):
        return up_hbm.at[pl.ds(pl.multiple_of(p * piece, piece), piece), :]

    def dn_part(j, k, other):
        side = ((1 - y) if other else y) * (H // 2)
        if j < DC - 1:
            return pl.ds(pl.multiple_of(side + k * depth, depth), depth), pl.ds(0, CW)
        return pl.ds(pl.multiple_of(side + k % 2 * 2 * depth, 2 * depth), 2 * depth), pl.ds(k // 2 * HALF, HALF)

    def dn_slot(s, j, k, other=False):
        r, c = dn_part(j, k, other)
        return dnw.at[s * DC + j, r, c]

    def dn_own(j, k, other=False):
        r, c = dn_part(j, k, other)
        return dn_hbm.at[r, pl.ds(j * CW + c.start, c.size)]

    def rank(s, where, here=False):
        plane = z if here or where is ACROSS else mate if where is MATE else inner
        return s - jnp.where(s > plane, 1, 0)

    def up_copy(s, p, src, where, other=False, here=False):
        slot = up_slot(s, p + ((1 - y) if other else y) * UM)
        crossing = where is ACROSS or other
        g = rank(s, where, here)
        recv = up_recv.at[(n - 1) * UM + g] if crossing else up_recv.at[g * UM + p]
        return remote(slot if src is None else src, slot, up_send.at[0], recv, where)

    def dn_copy(s, j, k, where, other=False, stored=False, here=False):
        slot = dn_slot(s, j, k, other)
        g = rank(s, where, here)
        if where is ACROSS or other:
            recv = dn_recv.at[(n - 1) * DC * DM + g * (DC + 1) + j + (k // 2 if j == DC - 1 else 0)]
        else:
            recv = dn_recv.at[(g * DC + j) * DM + k]
        return remote(dn_own(j, k, other) if stored else slot, slot, dn_send.at[0], recv, where)

    def up_landed(s, p):
        up_copy(s, p, None, MATE, here=True).wait_recv()

    def up_others(s):
        half = up_rows // 2
        ref = upw.at[pl.ds(pl.multiple_of(s * up_rows + (1 - y) * half, half), half), :]
        remote(ref, ref, up_send.at[0], up_recv.at[(n - 1) * UM + rank(s, MATE, True)], MATE).wait_recv()

    def dn_landed(s, j, k):
        dn_copy(s, j, k, MATE, here=True).wait_recv()

    def dn_others(s, j, h=0):
        cols = pl.ds(h * HALF, HALF) if j == DC - 1 else pl.ds(0, CW)
        ref = dnw.at[s * DC + j, pl.ds(pl.multiple_of((1 - y) * (H // 2), H // 2), H // 2), cols]
        recv = dn_recv.at[(n - 1) * DC * DM + rank(s, MATE, True) * (DC + 1) + j + h]
        remote(ref, ref, dn_send.at[0], recv, MATE).wait_recv()

    def tok_slot(q, b):
        return tok.at[1, pl.ds(pl.multiple_of(q * own_rows + b * band, band), band), :]

    def tok_copy(recv, q, b, src, where):
        return remote(src, tok_slot(q, b), t_send.at[0], t_recv.at[recv], where)

    def tok_all(recv, q):
        ref = tok.at[1, pl.ds(pl.multiple_of(q * own_rows, own_rows), own_rows), :]
        remote(ref, ref, t_send.at[0], t_recv.at[recv], MATE).wait_recv()

    def sent(ref, sem, where):
        remote(ref, ref, sem.at[0], sem.at[0], where).wait_send()

    def column(i):
        return unit[ORDER[i][0]] * DC + ORDER[i][1]

    def cut(h):
        return pl.ds(0, CW) if h is None else pl.ds(h * HALF, HALF)

    def mark(i, h):
        return chunks if h == 1 else i

    def out_part(q, h):
        start = pl.multiple_of(q * CW + (h or 0) * HALF, HALF)
        return out_hbm.at[:, pl.ds(start, CW if h is None else HALF)]

    def own_copy(i, h=None):
        q = column(i)
        return pltpu.make_async_copy(outv.at[0, q, :, cut(h)], out_part(q, h), own_sem.at[0])

    def own_done(count):
        width = pl.ds(0, count * CW)
        pltpu.make_async_copy(tok.at[0, pl.ds(0, own_rows), width], out_hbm.at[:, width], own_sem.at[0]).wait()

    def out_copy(i, h=None):
        q = column(i)
        return remote(outv.at[1, q, :, cut(h)], out_part(q, h), o_send.at[0], o_recv.at[mark(i, h)], OUTER)

    def d_copy(i, to, of, h=None):
        return remote(dsend.at[i, to, :, cut(h)], drecv.at[i, of, :, cut(h)], d_send.at[0], o_recv.at[mark(i, h)],
                      at(y, outer, to * 2 + core))

    def d_landed(i, h=None):
        ref = drecv.at[i, :, :, cut(h)]
        remote(ref, ref, d_send.at[0], o_recv.at[mark(i, h)], INNER).wait_recv()

    barrier = pltpu.get_barrier_semaphore()

    def greet(peers):
        for peer in peers:
            pl.semaphore_signal(barrier, inc=1, device_id=peer, device_id_type=pl.DeviceIdType.MESH)

    mine_up, other_up = y * UM, (1 - y) * UM
    passed = len(DIRECT)
    own_block = pl.ds(pl.multiple_of(t * own_rows, own_rows), own_rows)

    def own_tokens(src, q, h=None):
        start = pl.multiple_of(q * CW + (h or 0) * HALF, HALF)
        return tok[src, own_block, pl.ds(start, CW if h is None else HALF)].astype(jnp.float32)

    @pl.when(is_outer)
    def _():
        greet([INNER, at(y, inner, (1 - x) * 2 + core)])
        load = pltpu.make_async_copy(tok_hbm.at[own_block, :], tok.at[0, own_block, :], local.at[0])
        load.start()
        up_load = pltpu.make_async_copy(
            up_hbm, upw.at[pl.ds(pl.multiple_of(z * up_rows, up_rows), up_rows), :], local.at[2]
        )
        up_load.start()
        pl.semaphore_wait(barrier, 2)
        up_load.wait()
        for p in range(UM):
            up_copy(z, p, None, INNER).start()
        for b in range(TP):
            own = tok_hbm.at[pl.ds(pl.multiple_of(t * own_rows + b * band, band), band), :]
            tok_copy(b, t, b, own, INNER).start()
        for p in range(UM - BESIDE):
            up_copy(z, p, None, INNER, True).start()
        for other in (False, True):
            for j in range(DC):
                for k in range(DM):
                    dn_copy(z, j, k, INNER, other, True).start()
        load.wait()
        for i in range(chunks):
            for h in (0, 1) if i == chunks - 1 else (None,):
                if i in DIRECT:
                    d_landed(i, h)
                    q, c = column(i), cut(h)
                    res = own_tokens(0, q, h) + drecv[i, 0, :, c].astype(jnp.float32)
                    outv[0, q, :, c] = (res + drecv[i, 1, :, c].astype(jnp.float32)).astype(jnp.bfloat16)
                    own_copy(i, h).start()
                else:
                    out_copy(i, h).wait_recv()
        sent(upw.at[pl.ds(0, (2 * UM - BESIDE) * piece), :], up_send, INNER)
        sent(dnw.at[pl.ds(0, DC)], dn_send, INNER)
        sent(tok.at[0, pl.ds(0, own_rows), :], t_send, INNER)
        own_done(passed)

    @pl.when(jnp.logical_not(is_outer))
    def _():
        greet([PARTNER, ASIDE, ACROSS, MATE, OUTER, at(y, outer, (1 - x) * 2 + core)])
        tok_load = pltpu.make_async_copy(tok_hbm, tok.at[0], local.at[0])
        gain_load = pltpu.make_async_copy(gain_hbm, gain_ref, local.at[1])
        up_load = pltpu.make_async_copy(
            up_hbm, upw.at[pl.ds(pl.multiple_of(z * up_rows, up_rows), up_rows), :], local.at[2]
        )
        dn_loads = [
            pltpu.make_async_copy(dn_hbm.at[:, pl.ds(j * CW, CW)], dnw.at[z * DC + j], local.at[3 + j])
            for j in range(DC)
        ]
        for load in [up_load, gain_load, tok_load] + dn_loads:
            load.start()
        pl.semaphore_wait(barrier, 6)

        up_load.wait()
        for p in range(UM):
            up_copy(z, p, None, MATE).start()

        gain_load.wait()
        gain = gain_ref[...]

        def normalise(src, q):
            xf = tok[src, pl.ds(pl.multiple_of(q * own_rows, own_rows), own_rows), :].astype(jnp.float32)
            scale = lax.rsqrt(jnp.mean(xf * xf, axis=-1, keepdims=True) + EPS)
            to = (q % 2 * 2 + q // 2) * own_rows
            nrm[src, pl.ds(pl.multiple_of(to, own_rows), own_rows), :] = (xf * scale * gain).astype(jnp.bfloat16)

        def lift(src, start, size, first=False, last=False):
            k = pl.ds(pl.multiple_of(start, size), size)
            value = jnp.dot(nrm[src, :, k], upw[k, :], preferred_element_type=jnp.float32)
            if not first:
                value = value + lifted[src]
            if last:
                hid[src] = jnp.square(jnp.maximum(value, 0.0)).astype(jnp.bfloat16).reshape(2, rows // 2, H)
            else:
                lifted[src] = value

        def lift_mine(s):
            lift(0, s * up_rows + y * (up_rows // 2), up_rows // 2)

        def lift_others(s, last=False):
            up_others(s)
            lift(0, s * up_rows + (1 - y) * (up_rows // 2), up_rows // 2, last=last)

        def relay(name, j, k):
            s = unit[name]
            dn_landed(s, j, k)
            dn_copy(s, j, k, MATE if name == "outer" else ACROSS).start()

        def relay_up(s, p, where):
            up_copy(s, p, None, where).start()

        tok_load.wait()
        lax.fori_loop(0, 4, lambda q, carry: (normalise(0, q), carry)[1], 0)

        for p in range(UM):
            up_landed(outer, p)
            relay_up(outer, p, MATE)
            up_landed(mate, p)
            if p < UM - VIA_MATE:
                relay_up(mate, p, ACROSS)
            if p >= UM - BESIDE:
                relay_up(outer, p, ACROSS)
            if p == 1:
                lift(0, z * up_rows, up_rows, first=True)
        for p in range(UM - VIA_MATE, UM):
            up_copy(z, p, None, MATE, True).start()
        for j in range(DC):
            dn_loads[j].wait()
            for k in range(DM):
                dn_copy(z, j, k, MATE, False, True).start()
        lift_mine(outer)
        lift_mine(mate)

        beside, beyond = x * 2 + 1 - core, (1 - x) * 2 + core
        corner = (1 - x) * 2 + 1 - core

        def pass_beyond(b):
            tok_copy(TP + b, beyond, b, tok_slot(beyond, b), ASIDE).wait_recv()
            tok_copy(2 * TP + 1, beyond, b, tok_slot(beyond, b), PARTNER).start()

        for b in range(TP):
            for p in range(b * UM // TP, (b + 1) * UM // TP):
                up_landed(far, p)
                relay_up(far, p, ACROSS)
            tok_copy(b, t, b, tok_slot(t, b), INNER).wait_recv()
            tok_copy(TP + b, t, b, tok_slot(t, b), ASIDE).start()
            tok_copy(2 * TP, t, b, tok_slot(t, b), PARTNER).start()
            if b > 1:
                pass_beyond(b - 2)
        due = []
        for name, first in (("mate", 32.2), ("outer", 34.0), ("far", 43.5)):
            due += [(first + 1.4 * q, name, q // DM, q % DM) for q in range(DC * DM)]
        due.sort()

        def relays(until):
            while due and due[0][0] <= until:
                relay(*due.pop(0)[1:])

        normalise(1, t)
        lift_mine(far)
        tok_all(2 * TP, beside)
        normalise(1, beside)
        pass_beyond(TP - 2)
        pass_beyond(TP - 1)
        normalise(1, beyond)
        relays(33)
        tok_all(2 * TP + 1, corner)
        normalise(1, corner)
        near = jnp.where(z < n // 2, 0, n // 2) * up_rows
        lift_others(outer)
        relays(33.7)
        lift(1, near, 2 * up_rows, first=True)
        relays(35)
        lift_others(mate)
        relays(35.5)
        lift_others(far, last=True)
        relays(36.5)
        lift(1, (n // 2) * up_rows - near, 2 * up_rows, last=True)
        relays(37.8)

        def a_copy(i, src, h=None):
            return remote(asend.at[i, src, :, :, cut(h)], arecv.at[i, src, :, :, cut(h)],
                          a_send.at[0], a_recv.at[mark(i, h), src], PARTNER)

        def b_copy(i, src, h=None):
            return remote(bsend.at[i, src, :, cut(h)], brecv.at[i, src, :, cut(h)],
                          b_send.at[0], b_recv.at[mark(i, h), src], ASIDE)

        joining, finishing = [], []

        def join(left=0):
            while len(joining) > left:
                i, src, h = joining.pop(0)
                c = cut(h)
                a_copy(i, src, h).wait_recv()

                def added(to):
                    return part[i % 2, src, core, to, :, c] + arecv[i, src, to, :, c].astype(jnp.float32)

                if src == 1 and i in DIRECT:
                    for to in (1 - x, x):
                        dsend[i, to, :, c] = added(to).astype(jnp.bfloat16)
                        d_copy(i, to, x, h).start()
                else:
                    bsend[i, src, :, c] = added(1 - x).astype(jnp.bfloat16)
                    b_copy(i, src, h).start()
                    keep[i, src, :, c] = added(x)
                    finishing.append((i, src, h))

        def pick(*item):
            joining.remove(item)
            joining.insert(0, item)
            join(len(joining) - 1)

        def finish(left):
            while len(finishing) > left:
                i, src, h = finishing.pop(0)
                q, c = column(i), cut(h)
                b_copy(i, src, h).wait_recv()
                res = own_tokens(src, q, h) + keep[i, src, :, c] + brecv[i, src, :, c].astype(jnp.float32)
                outv[src, q, :, c] = res.astype(jnp.bfloat16)
                (own_copy if src == 0 else out_copy)(i, h).start()

        def give(i, src, h=None):
            c = cut(h)
            asend[i, src, :, :, c] = part[i % 2, src, 1 - core, :, :, c].astype(jnp.bfloat16)
            a_copy(i, src, h).start()
            joining.append((i, src, h))

        def arrive(i):
            name, j = ORDER[i]
            if name != "inner":
                for h in (0, 1) if j == DC - 1 else (0,):
                    dn_others(unit[name], j, h)

        def compute(i, src, h=None):
            block = dnw[column(i), :, cut(h)]
            for side in (0, 1):
                product = jnp.dot(hid[src, side], block, preferred_element_type=jnp.float32)
                part[i % 2, src, side, :, :, cut(h)] = product.reshape(2, own_rows, block.shape[1])
            give(i, src, h)

        def both(i, h=None):
            block = dnw[column(i), :, cut(h)]
            for src in (0, 1):
                product = jnp.dot(hid[src].reshape(rows, H), block, preferred_element_type=jnp.float32)
                part[i % 2, src, :, :, :, cut(h)] = product.reshape(2, 2, own_rows, block.shape[1])
            give(i, 1, h)
            give(i, 0, h)

        both(0)
        relays(39.2)
        both(1)
        join(2)
        relays(40.6)
        join()
        relays(42)
        arrive(2)
        both(2)
        relays(43.6)
        join()
        relays(46.4)
        finish(3)
        arrive(3)
        both(3)
        relays(47.8)
        finish(2)
        join()
        relays(49.2)
        finish(2)
        arrive(4)
        both(4)
        relays(50.6)
        join()
        relays(52)
        relays(99)
        arrive(5)
        both(5)
        finish(1)
        arrive(6)
        compute(6, 1)
        join(1)
        compute(6, 0)
        finish(2)
        dn_others(far, DC - 1, 0)
        both(7, 0)
        pick(6, 1, None)
        dn_others(far, DC - 1, 1)
        compute(7, 1, 1)
        pick(7, 1, 0)
        compute(7, 0, 1)
        pick(7, 1, 1)
        finish(0)
        join()
        finish(0)

        ups = 2 * UM + VIA_MATE + (UM - VIA_MATE) + UM + BESIDE
        sent(upw.at[pl.ds(0, ups * piece), :], up_send, MATE)
        sent(dnw.at[pl.ds(0, 2 * DC)], dn_send, MATE)
        sent(tok.at[0, pl.ds(0, 3 * own_rows), :], t_send, MATE)
        sent(asend, a_send, PARTNER)
        sent(bsend.at[pl.ds(0, chunks - passed // 2)], b_send, ASIDE)
        sent(outv.at[1, pl.ds(0, chunks - passed)], o_send, OUTER)
        sent(dsend.at[pl.ds(0, passed)], d_send, OUTER)
        own_done(chunks)


def fused(n, tokens, norm_gain, up_weight, down_weight):
    rows, D = tokens.shape
    up_rows, H = up_weight.shape
    CW = down_weight.shape[1] // DN_CHUNKS
    chunks = n * DN_CHUNKS
    own_rows = rows // 4
    bf, f32 = jnp.bfloat16, jnp.float32
    dma = pltpu.SemaphoreType.DMA
    return pl.pallas_call(
        functools.partial(kernel, n),
        out_shape=jax.ShapeDtypeStruct((own_rows, D), bf),
        in_specs=[pl.BlockSpec(memory_space=pl.ANY)] * 4,
        out_specs=pl.BlockSpec(memory_space=pl.ANY),
        scratch_shapes=[
            pltpu.VMEM((1, D), f32),
            pltpu.VMEM((2, rows, D), bf),
            pltpu.VMEM((2, rows, D), bf),
            pltpu.VMEM((n * up_rows, H), bf),
            pltpu.VMEM((chunks, H, CW), bf),
            pltpu.VMEM((2, rows, H), f32),
            pltpu.VMEM((2, 2, rows // 2, H), bf),
            pltpu.VMEM((2, 2, 2, 2, own_rows, CW), f32),
            pltpu.VMEM((chunks, 2, 2, own_rows, CW), bf),
            pltpu.VMEM((chunks, 2, 2, own_rows, CW), bf),
            pltpu.VMEM((chunks, 2, own_rows, CW), bf),
            pltpu.VMEM((chunks, 2, own_rows, CW), bf),
            pltpu.VMEM((chunks, 2, own_rows, CW), f32),
            pltpu.VMEM((2, chunks, own_rows, CW), bf),
            pltpu.VMEM((chunks, 2, own_rows, CW), bf),
            pltpu.VMEM((chunks, 2, own_rows, CW), bf),
            dma((1,)),
            dma(((n - 1) * (UP_PIECES // 2 + 1),)),
            dma((1,)),
            dma(((n - 1) * (DN_CHUNKS * (DN_PIECES // 2 + 1) + 1),)),
            dma((1,)),
            dma((2 * TOK_PIECES + 2,)),
            dma((1,)),
            dma((chunks + 1, 2)),
            dma((1,)),
            dma((chunks + 1, 2)),
            dma((1,)),
            dma((chunks + 1,)),
            dma((1,)),
            dma((1,)),
            dma((3 + DN_CHUNKS,)),
        ],
        compiler_params=pltpu.CompilerParams(
            collective_id=0, has_side_effects=True, vmem_limit_bytes=53 * 1024 * 1024
        ),
    )(tokens, norm_gain.reshape(1, D), up_weight, down_weight)


def fits(mesh, tokens, up_weight, down_weight):
    n = mesh.shape["fs"]
    rows = tokens.shape[0] // (mesh.shape["rep"] * n)
    columns = down_weight.shape[1] // n
    depth = up_weight.shape[0] // n
    hidden = up_weight.shape[1] // mesh.shape["tp"]
    return (
        mesh.shape["rep"] == 2
        and mesh.shape["tp"] == 4
        and n == 4
        and columns % (256 * DN_CHUNKS) == 0
        and depth % (UP_PIECES * 16) == 0
        and depth % 128 == 0
        and hidden % (16 * DN_PIECES) == 0
        and hidden % 128 == 0
        and rows % (4 * 16 * TOK_PIECES) == 0
        and rows <= 512
        and hidden <= 1024
        and tokens.shape[1] <= 2048
    )


def solution(mesh):
    placed = (P(("rep", "fs"), None), P(), P("fs", "tp"), P("tp", "fs"))

    def layer(tokens, norm_gain, up_weight, down_weight):
        if fits(mesh, tokens, up_weight, down_weight):
            body = functools.partial(fused, mesh.shape["fs"])
        else:
            body = shards
        return jax.shard_map(
            body, mesh=mesh, in_specs=placed, out_specs=P(("rep", "fs", "tp"), None), check_vma=False
        )(tokens, norm_gain, up_weight, down_weight)

    return layer
```

```python
import functools

import jax
import jax.numpy as jnp
from jax import lax
from jax.experimental import pallas as pl
from jax.experimental.pallas import tpu as pltpu
from jax.sharding import PartitionSpec as P

EPS = 1e-06
UP_PIECES = 16
DN_CHUNKS = 2
DN_PIECES = 8
TOK_PIECES = 4
BESIDE = 4
VIA_MATE = 2
LAG = 4
ORDER = (
    ("inner", 0), ("inner", 1), ("mate", 0), ("mate", 1),
    ("outer", 0), ("far", 0), ("outer", 1), ("far", 1),
)
DIRECT = (1, 2, 3, 4, 5, 7)


def shards(tokens, norm_gain, up_weight, down_weight):
    xf = tokens.astype(jnp.float32)
    scale = lax.rsqrt(jnp.mean(xf * xf, axis=-1, keepdims=True) + EPS)
    normed = (xf * scale * norm_gain).astype(jnp.bfloat16)
    rows = tokens.shape[0]
    halves = lax.axis_size("rep")
    share = up_weight.shape[0] // halves
    mine = lax.dynamic_slice_in_dim(up_weight, lax.axis_index("rep") * share, share, 0)
    arranged = normed.reshape(rows, -1, halves, share).transpose(0, 2, 1, 3).reshape(rows, -1)
    lifted = jnp.dot(
        arranged,
        lax.all_gather(mine, ("rep", "fs"), axis=0, tiled=True),
        preferred_element_type=jnp.float32,
    )
    width = down_weight.shape[1] // halves
    down_mine = lax.dynamic_slice_in_dim(down_weight, lax.axis_index("rep") * width, width, 1)
    collected = lax.all_gather(down_mine, ("rep", "fs"), axis=1, tiled=True)
    hidden_rows = collected.shape[0]
    down_block = (
        collected.reshape(hidden_rows, halves, -1, width)
        .transpose(0, 2, 1, 3)
        .reshape(hidden_rows, -1)
    )
    hidden = jnp.square(jnp.maximum(lifted, 0.0)).astype(jnp.bfloat16)
    own_rows = rows // lax.axis_size("tp")
    summed = lax.psum_scatter(
        jnp.dot(hidden, down_block, preferred_element_type=jnp.float32).astype(jnp.bfloat16),
        "tp",
        scatter_dimension=0,
        tiled=True,
    ).astype(jnp.float32)
    residual = lax.dynamic_slice_in_dim(xf, lax.axis_index("tp") * own_rows, own_rows, 0)
    return (residual + summed).astype(jnp.bfloat16)


def kernel(
    n, tok_hbm, gain_hbm, up_hbm, dn_hbm, out_hbm,
    gain_ref, tok, nrm, upw, dnw, lifted, hid, part, asend, arecv, bsend, brecv, keep, outv, dsend, drecv,
    up_send, up_recv, dn_send, dn_recv, t_send, t_recv,
    a_send, a_recv, b_send, b_recv, o_send, o_recv, d_send, own_sem, local,
):
    y, z, t = lax.axis_index("rep"), lax.axis_index("fs"), lax.axis_index("tp")
    x, core = t // 2, t % 2
    rows = tok_hbm.shape[0]
    own_rows = rows // 4
    up_rows, H = up_hbm.shape
    CW = dnw.shape[2]
    UP, DC, DP, TP = UP_PIECES, DN_CHUNKS, DN_PIECES, TOK_PIECES
    UM, DM = UP // 2, DP // 2
    piece, depth, band = up_rows // UP, H // DP, own_rows // TP
    chunks = n * DC
    HALF = CW // 2

    is_outer = (z == 0) | (z == n - 1)
    outer = jnp.where(z < n // 2, 0, n - 1)
    inner = jnp.where(z < n // 2, n // 2 - 1, n // 2)
    mate = n - 1 - inner
    far = n - 1 - outer
    unit = {"inner": inner, "mate": mate, "outer": outer, "far": far}

    def at(yy, zz, tt):
        return {"rep": yy, "fs": zz, "tp": tt}

    PARTNER = at(y, z, x * 2 + (1 - core))
    ASIDE = at(y, z, (1 - x) * 2 + core)
    ACROSS = at(1 - y, z, t)
    MATE = at(y, mate, t)
    OUTER = at(y, outer, t)
    INNER = at(y, inner, t)

    def remote(src, dst, send, recv, where):
        return pltpu.make_async_remote_copy(
            src_ref=src, dst_ref=dst, send_sem=send, recv_sem=recv,
            device_id=where, device_id_type=pl.DeviceIdType.MESH,
        )

    def up_slot(s, p):
        return upw.at[pl.ds(pl.multiple_of(s * up_rows + p * piece, piece), piece), :]

    def up_own(p):
        return up_hbm.at[pl.ds(pl.multiple_of(p * piece, piece), piece), :]

    def dn_part(j, k, other):
        side = ((1 - y) if other else y) * (H // 2)
        if j < DC - 1:
            return pl.ds(pl.multiple_of(side + k * depth, depth), depth), pl.ds(0, CW)
        return pl.ds(pl.multiple_of(side + k % 2 * 2 * depth, 2 * depth), 2 * depth), pl.ds(k // 2 * HALF, HALF)

    def dn_slot(s, j, k, other=False):
        r, c = dn_part(j, k, other)
        return dnw.at[s * DC + j, r, c]

    def dn_own(j, k, other=False):
        r, c = dn_part(j, k, other)
        return dn_hbm.at[r, pl.ds(j * CW + c.start, c.size)]

    def rank(s, where, here=False):
        plane = z if here or where is ACROSS else mate if where is MATE else inner
        return s - jnp.where(s > plane, 1, 0)

    def up_copy(s, p, src, where, other=False, here=False):
        slot = up_slot(s, p + ((1 - y) if other else y) * UM)
        crossing = where is ACROSS or other
        g = rank(s, where, here)
        recv = up_recv.at[(n - 1) * UM + g] if crossing else up_recv.at[g * UM + p]
        return remote(slot if src is None else src, slot, up_send.at[0], recv, where)

    def dn_copy(s, j, k, where, other=False, stored=False, here=False):
        slot = dn_slot(s, j, k, other)
        g = rank(s, where, here)
        if where is ACROSS or other:
            recv = dn_recv.at[(n - 1) * DC * DM + g * (DC + 1) + j + (k // 2 if j == DC - 1 else 0)]
        else:
            recv = dn_recv.at[(g * DC + j) * DM + k]
        return remote(dn_own(j, k, other) if stored else slot, slot, dn_send.at[0], recv, where)

    def up_landed(s, p):
        up_copy(s, p, None, MATE, here=True).wait_recv()

    def up_others(s):
        half = up_rows // 2
        ref = upw.at[pl.ds(pl.multiple_of(s * up_rows + (1 - y) * half, half), half), :]
        remote(ref, ref, up_send.at[0], up_recv.at[(n - 1) * UM + rank(s, MATE, True)], MATE).wait_recv()

    def dn_landed(s, j, k):
        dn_copy(s, j, k, MATE, here=True).wait_recv()

    def dn_others(s, j, h=0):
        cols = pl.ds(h * HALF, HALF) if j == DC - 1 else pl.ds(0, CW)
        ref = dnw.at[s * DC + j, pl.ds(pl.multiple_of((1 - y) * (H // 2), H // 2), H // 2), cols]
        recv = dn_recv.at[(n - 1) * DC * DM + rank(s, MATE, True) * (DC + 1) + j + h]
        remote(ref, ref, dn_send.at[0], recv, MATE).wait_recv()

    def tok_slot(q, b):
        return tok.at[1, pl.ds(pl.multiple_of(q * own_rows + b * band, band), band), :]

    def tok_copy(recv, q, b, src, where):
        return remote(src, tok_slot(q, b), t_send.at[0], t_recv.at[recv], where)

    def tok_all(recv, q):
        ref = tok.at[1, pl.ds(pl.multiple_of(q * own_rows, own_rows), own_rows), :]
        remote(ref, ref, t_send.at[0], t_recv.at[recv], MATE).wait_recv()

    def sent(ref, sem, where):
        remote(ref, ref, sem.at[0], sem.at[0], where).wait_send()

    def column(i):
        return unit[ORDER[i][0]] * DC + ORDER[i][1]

    def cut(h):
        return pl.ds(0, CW) if h is None else pl.ds(h * HALF, HALF)

    def mark(i, h):
        return chunks if h == 1 else i

    def out_part(q, h):
        start = pl.multiple_of(q * CW + (h or 0) * HALF, HALF)
        return out_hbm.at[:, pl.ds(start, CW if h is None else HALF)]

    def own_copy(i, h=None):
        q = column(i)
        return pltpu.make_async_copy(outv.at[0, q, :, cut(h)], out_part(q, h), own_sem.at[0])

    def own_done(count):
        width = pl.ds(0, count * CW)
        pltpu.make_async_copy(tok.at[0, pl.ds(0, own_rows), width], out_hbm.at[:, width], own_sem.at[0]).wait()

    def out_copy(i, h=None):
        q = column(i)
        return remote(outv.at[1, q, :, cut(h)], out_part(q, h), o_send.at[0], o_recv.at[mark(i, h)], OUTER)

    def d_copy(i, to, of, h=None):
        return remote(dsend.at[i, to, :, cut(h)], drecv.at[i, of, :, cut(h)], d_send.at[0], o_recv.at[mark(i, h)],
                      at(y, outer, to * 2 + core))

    def d_landed(i, h=None):
        ref = drecv.at[i, :, :, cut(h)]
        remote(ref, ref, d_send.at[0], o_recv.at[mark(i, h)], INNER).wait_recv()

    barrier = pltpu.get_barrier_semaphore()

    def greet(peers):
        for peer in peers:
            pl.semaphore_signal(barrier, inc=1, device_id=peer, device_id_type=pl.DeviceIdType.MESH)

    mine_up, other_up = y * UM, (1 - y) * UM
    passed = len(DIRECT)
    own_block = pl.ds(pl.multiple_of(t * own_rows, own_rows), own_rows)

    def own_tokens(src, q, h=None):
        start = pl.multiple_of(q * CW + (h or 0) * HALF, HALF)
        return tok[src, own_block, pl.ds(start, CW if h is None else HALF)].astype(jnp.float32)

    @pl.when(is_outer)
    def _():
        greet([INNER, at(y, inner, (1 - x) * 2 + core)])
        load = pltpu.make_async_copy(tok_hbm.at[own_block, :], tok.at[0, own_block, :], local.at[0])
        load.start()
        up_load = pltpu.make_async_copy(
            up_hbm, upw.at[pl.ds(pl.multiple_of(z * up_rows, up_rows), up_rows), :], local.at[2]
        )
        up_load.start()
        pl.semaphore_wait(barrier, 2)
        up_load.wait()
        for p in range(UM):
            up_copy(z, p, None, INNER).start()
        for b in range(TP):
            own = tok_hbm.at[pl.ds(pl.multiple_of(t * own_rows + b * band, band), band), :]
            tok_copy(b, t, b, own, INNER).start()
        for p in range(UM - BESIDE):
            up_copy(z, p, None, INNER, True).start()
        for other in (False, True):
            for j in range(DC):
                for k in range(DM):
                    dn_copy(z, j, k, INNER, other, True).start()
        load.wait()
        for i in range(chunks):
            for h in (0, 1) if i == chunks - 1 else (None,):
                if i in DIRECT:
                    d_landed(i, h)
                    q, c = column(i), cut(h)
                    res = own_tokens(0, q, h) + drecv[i, 0, :, c].astype(jnp.float32)
                    outv[0, q, :, c] = (res + drecv[i, 1, :, c].astype(jnp.float32)).astype(jnp.bfloat16)
                    own_copy(i, h).start()
                else:
                    out_copy(i, h).wait_recv()
        sent(upw.at[pl.ds(0, (2 * UM - BESIDE) * piece), :], up_send, INNER)
        sent(dnw.at[pl.ds(0, DC)], dn_send, INNER)
        sent(tok.at[0, pl.ds(0, own_rows), :], t_send, INNER)
        own_done(passed)

    @pl.when(jnp.logical_not(is_outer))
    def _():
        greet([PARTNER, ASIDE, ACROSS, MATE, OUTER, at(y, outer, (1 - x) * 2 + core)])
        tok_load = pltpu.make_async_copy(tok_hbm, tok.at[0], local.at[0])
        gain_load = pltpu.make_async_copy(gain_hbm, gain_ref, local.at[1])
        up_load = pltpu.make_async_copy(
            up_hbm, upw.at[pl.ds(pl.multiple_of(z * up_rows, up_rows), up_rows), :], local.at[2]
        )
        dn_loads = [
            pltpu.make_async_copy(dn_hbm.at[:, pl.ds(j * CW, CW)], dnw.at[z * DC + j], local.at[3 + j])
            for j in range(DC)
        ]
        for load in [up_load, gain_load, tok_load] + dn_loads:
            load.start()
        pl.semaphore_wait(barrier, 6)

        up_load.wait()
        for p in range(UM):
            up_copy(z, p, None, MATE).start()

        gain_load.wait()
        gain = gain_ref[...]

        def normalise(src, q):
            xf = tok[src, pl.ds(pl.multiple_of(q * own_rows, own_rows), own_rows), :].astype(jnp.float32)
            scale = lax.rsqrt(jnp.mean(xf * xf, axis=-1, keepdims=True) + EPS)
            to = (q % 2 * 2 + q // 2) * own_rows
            nrm[src, pl.ds(pl.multiple_of(to, own_rows), own_rows), :] = (xf * scale * gain).astype(jnp.bfloat16)

        def lift(src, start, size, first=False, last=False):
            k = pl.ds(pl.multiple_of(start, size), size)
            value = jnp.dot(nrm[src, :, k], upw[k, :], preferred_element_type=jnp.float32)
            if not first:
                value = value + lifted[src]
            if last:
                hid[src] = jnp.square(jnp.maximum(value, 0.0)).astype(jnp.bfloat16).reshape(2, rows // 2, H)
            else:
                lifted[src] = value

        def lift_mine(s):
            lift(0, s * up_rows + y * (up_rows // 2), up_rows // 2)

        def lift_others(s, last=False):
            up_others(s)
            lift(0, s * up_rows + (1 - y) * (up_rows // 2), up_rows // 2, last=last)

        def relay(name, j, k):
            s = unit[name]
            dn_landed(s, j, k)
            dn_copy(s, j, k, MATE if name == "outer" else ACROSS).start()

        def relay_up(s, p, where):
            up_copy(s, p, None, where).start()

        tok_load.wait()
        lax.fori_loop(0, 4, lambda q, carry: (normalise(0, q), carry)[1], 0)

        for p in range(UM):
            up_landed(outer, p)
            relay_up(outer, p, MATE)
            up_landed(mate, p)
            if p < UM - VIA_MATE:
                relay_up(mate, p, ACROSS)
            if p >= UM - BESIDE:
                relay_up(outer, p, ACROSS)
            if p == 1:
                lift(0, z * up_rows, up_rows, first=True)
        for p in range(UM - VIA_MATE, UM):
            up_copy(z, p, None, MATE, True).start()
        for j in range(DC):
            dn_loads[j].wait()
            for k in range(DM):
                dn_copy(z, j, k, MATE, False, True).start()
        lift_mine(outer)
        lift_mine(mate)

        beside, beyond = x * 2 + 1 - core, (1 - x) * 2 + core
        corner = (1 - x) * 2 + 1 - core

        def pass_beyond(b):
            tok_copy(TP + b, beyond, b, tok_slot(beyond, b), ASIDE).wait_recv()
            tok_copy(2 * TP + 1, beyond, b, tok_slot(beyond, b), PARTNER).start()

        for b in range(TP):
            for p in range(b * UM // TP, (b + 1) * UM // TP):
                up_landed(far, p)
                relay_up(far, p, ACROSS)
            tok_copy(b, t, b, tok_slot(t, b), INNER).wait_recv()
            tok_copy(TP + b, t, b, tok_slot(t, b), ASIDE).start()
            tok_copy(2 * TP, t, b, tok_slot(t, b), PARTNER).start()
            if b > 1:
                pass_beyond(b - 2)
        due = []
        for name, first in (("mate", 32.2), ("outer", 34.0), ("far", 43.5)):
            due += [(first + 1.4 * q, name, q // DM, q % DM) for q in range(DC * DM)]
        due.sort()

        def relays(until):
            while due and due[0][0] <= until:
                relay(*due.pop(0)[1:])

        normalise(1, t)
        lift_mine(far)
        tok_all(2 * TP, beside)
        normalise(1, beside)
        pass_beyond(TP - 2)
        pass_beyond(TP - 1)
        normalise(1, beyond)
        relays(33)
        tok_all(2 * TP + 1, corner)
        normalise(1, corner)
        near = jnp.where(z < n // 2, 0, n // 2) * up_rows
        lift_others(outer)
        relays(33.7)
        lift(1, near, 2 * up_rows, first=True)
        relays(35)
        lift_others(mate)
        relays(35.5)
        lift_others(far, last=True)
        relays(36.5)
        lift(1, (n // 2) * up_rows - near, 2 * up_rows, last=True)
        relays(37.8)

        def a_copy(i, src, h=None):
            return remote(asend.at[i, src, :, :, cut(h)], arecv.at[i, src, :, :, cut(h)],
                          a_send.at[0], a_recv.at[mark(i, h), src], PARTNER)

        def b_copy(i, src, h=None):
            return remote(bsend.at[i, src, :, cut(h)], brecv.at[i, src, :, cut(h)],
                          b_send.at[0], b_recv.at[mark(i, h), src], ASIDE)

        joining, finishing = [], []

        def join(left=0):
            while len(joining) > left:
                i, src, h = joining.pop(0)
                c = cut(h)
                a_copy(i, src, h).wait_recv()

                def added(to):
                    return part[i % 2, src, core, to, :, c] + arecv[i, src, to, :, c].astype(jnp.float32)

                if src == 1 and i in DIRECT:
                    for to in (1 - x, x):
                        dsend[i, to, :, c] = added(to).astype(jnp.bfloat16)
                        d_copy(i, to, x, h).start()
                else:
                    bsend[i, src, :, c] = added(1 - x).astype(jnp.bfloat16)
                    b_copy(i, src, h).start()
                    keep[i, src, :, c] = added(x)
                    finishing.append((i, src, h))

        def pick(*item):
            joining.remove(item)
            joining.insert(0, item)
            join(len(joining) - 1)

        def finish(left):
            while len(finishing) > left:
                i, src, h = finishing.pop(0)
                q, c = column(i), cut(h)
                b_copy(i, src, h).wait_recv()
                res = own_tokens(src, q, h) + keep[i, src, :, c] + brecv[i, src, :, c].astype(jnp.float32)
                outv[src, q, :, c] = res.astype(jnp.bfloat16)
                (own_copy if src == 0 else out_copy)(i, h).start()

        def give(i, src, h=None):
            c = cut(h)
            asend[i, src, :, :, c] = part[i % 2, src, 1 - core, :, :, c].astype(jnp.bfloat16)
            a_copy(i, src, h).start()
            joining.append((i, src, h))

        def arrive(i):
            name, j = ORDER[i]
            if name != "inner":
                for h in (0, 1) if j == DC - 1 else (0,):
                    dn_others(unit[name], j, h)

        def compute(i, src, h=None):
            block = dnw[column(i), :, cut(h)]
            for side in (0, 1):
                product = jnp.dot(hid[src, side], block, preferred_element_type=jnp.float32)
                part[i % 2, src, side, :, :, cut(h)] = product.reshape(2, own_rows, block.shape[1])
            give(i, src, h)

        def both(i, h=None):
            block = dnw[column(i), :, cut(h)]
            for src in (0, 1):
                product = jnp.dot(hid[src].reshape(rows, H), block, preferred_element_type=jnp.float32)
                part[i % 2, src, :, :, :, cut(h)] = product.reshape(2, 2, own_rows, block.shape[1])
            give(i, 1, h)
            give(i, 0, h)

        both(0)
        relays(39.2)
        both(1)
        join(2)
        relays(40.6)
        join()
        relays(42)
        arrive(2)
        both(2)
        relays(43.6)
        join()
        relays(46.4)
        finish(3)
        arrive(3)
        both(3)
        relays(47.8)
        join()
        relays(49.2)
        arrive(4)
        both(4)
        relays(50.6)
        join()
        relays(52)
        relays(99)
        arrive(5)
        both(5)
        arrive(6)
        compute(6, 1)
        join(1)
        compute(6, 0)
        finish(2)
        dn_others(far, DC - 1, 0)
        both(7, 0)
        pick(6, 1, None)
        dn_others(far, DC - 1, 1)
        compute(7, 1, 1)
        pick(7, 1, 0)
        compute(7, 0, 1)
        pick(7, 1, 1)
        finish(0)
        join()
        finish(0)

        ups = 2 * UM + VIA_MATE + (UM - VIA_MATE) + UM + BESIDE
        sent(upw.at[pl.ds(0, ups * piece), :], up_send, MATE)
        sent(dnw.at[pl.ds(0, 2 * DC)], dn_send, MATE)
        sent(tok.at[0, pl.ds(0, 3 * own_rows), :], t_send, MATE)
        sent(asend, a_send, PARTNER)
        sent(bsend.at[pl.ds(0, chunks - passed // 2)], b_send, ASIDE)
        sent(outv.at[1, pl.ds(0, chunks - passed)], o_send, OUTER)
        sent(dsend.at[pl.ds(0, passed)], d_send, OUTER)
        own_done(chunks)


def fused(n, tokens, norm_gain, up_weight, down_weight):
    rows, D = tokens.shape
    up_rows, H = up_weight.shape
    CW = down_weight.shape[1] // DN_CHUNKS
    chunks = n * DN_CHUNKS
    own_rows = rows // 4
    bf, f32 = jnp.bfloat16, jnp.float32
    dma = pltpu.SemaphoreType.DMA
    return pl.pallas_call(
        functools.partial(kernel, n),
        out_shape=jax.ShapeDtypeStruct((own_rows, D), bf),
        in_specs=[pl.BlockSpec(memory_space=pl.ANY)] * 4,
        out_specs=pl.BlockSpec(memory_space=pl.ANY),
        scratch_shapes=[
            pltpu.VMEM((1, D), f32),
            pltpu.VMEM((2, rows, D), bf),
            pltpu.VMEM((2, rows, D), bf),
            pltpu.VMEM((n * up_rows, H), bf),
            pltpu.VMEM((chunks, H, CW), bf),
            pltpu.VMEM((2, rows, H), f32),
            pltpu.VMEM((2, 2, rows // 2, H), bf),
            pltpu.VMEM((2, 2, 2, 2, own_rows, CW), f32),
            pltpu.VMEM((chunks, 2, 2, own_rows, CW), bf),
            pltpu.VMEM((chunks, 2, 2, own_rows, CW), bf),
            pltpu.VMEM((chunks, 2, own_rows, CW), bf),
            pltpu.VMEM((chunks, 2, own_rows, CW), bf),
            pltpu.VMEM((chunks, 2, own_rows, CW), f32),
            pltpu.VMEM((2, chunks, own_rows, CW), bf),
            pltpu.VMEM((chunks, 2, own_rows, CW), bf),
            pltpu.VMEM((chunks, 2, own_rows, CW), bf),
            dma((1,)),
            dma(((n - 1) * (UP_PIECES // 2 + 1),)),
            dma((1,)),
            dma(((n - 1) * (DN_CHUNKS * (DN_PIECES // 2 + 1) + 1),)),
            dma((1,)),
            dma((2 * TOK_PIECES + 2,)),
            dma((1,)),
            dma((chunks + 1, 2)),
            dma((1,)),
            dma((chunks + 1, 2)),
            dma((1,)),
            dma((chunks + 1,)),
            dma((1,)),
            dma((1,)),
            dma((3 + DN_CHUNKS,)),
        ],
        compiler_params=pltpu.CompilerParams(
            collective_id=0, has_side_effects=True, vmem_limit_bytes=53 * 1024 * 1024
        ),
    )(tokens, norm_gain.reshape(1, D), up_weight, down_weight)


def fits(mesh, tokens, up_weight, down_weight):
    n = mesh.shape["fs"]
    rows = tokens.shape[0] // (mesh.shape["rep"] * n)
    columns = down_weight.shape[1] // n
    depth = up_weight.shape[0] // n
    hidden = up_weight.shape[1] // mesh.shape["tp"]
    return (
        mesh.shape["rep"] == 2
        and mesh.shape["tp"] == 4
        and n == 4
        and columns % (256 * DN_CHUNKS) == 0
        and depth % (UP_PIECES * 16) == 0
        and depth % 128 == 0
        and hidden % (16 * DN_PIECES) == 0
        and hidden % 128 == 0
        and rows % (4 * 16 * TOK_PIECES) == 0
        and rows <= 512
        and hidden <= 1024
        and tokens.shape[1] <= 2048
    )


def solution(mesh):
    placed = (P(("rep", "fs"), None), P(), P("fs", "tp"), P("tp", "fs"))

    def layer(tokens, norm_gain, up_weight, down_weight):
        if fits(mesh, tokens, up_weight, down_weight):
            body = functools.partial(fused, mesh.shape["fs"])
        else:
            body = shards
        return jax.shard_map(
            body, mesh=mesh, in_specs=placed, out_specs=P(("rep", "fs", "tp"), None), check_vma=False
        )(tokens, norm_gain, up_weight, down_weight)

    return layer
```
